256 devices in a mesh: sp: 64 (over z, x, core), tp: 4 (over y).
Axes of the slice: x: 4, y: 4, z: 8, core: 2. Of those that a mesh axis runs over, the one named last changes fastest.
Arguments:
- moe_input: bfloat16 [16384, 2048], P('sp'), may hold values from -6 to 6
- out_cotangent: bfloat16 [16384, 2048], P('sp'), may hold values from -16 to 16
- routes: int32 [16384, 2], P('sp'), may hold values from 0 to 63, all different within a row; in each aligned block of 256 rows (0 to 255, 256 to 511, ...) at most 12 rows name the same one
- group_weight: float32 [16384], P('sp'), may hold values from 0.5 to 1
- inner_weight: float32 [16384, 2], P('sp'), may hold values from 0.3 to 1
- gate_weight: bfloat16 [64, 2048, 1024], P('sp', None, 'tp'), may hold values from -0.125 to 0.125
- up_weight: bfloat16 [64, 2048, 1024], P('sp', None, 'tp'), may hold values from -0.125 to 0.125
- down_weight: bfloat16 [64, 1024, 2048], P('sp', 'tp'), may hold values from -0.1875 to 0.1875
- value_in: bfloat16 [16384, 1024], P('sp', 'tp'), may hold values from -6 to 6
- gate_in: bfloat16 [16384, 1024], P('sp', 'tp'), may hold values from -6 to 6
- conv_taps: bfloat16 [31, 1024], P(None, 'tp'), may hold values from -1 to 1
- norm_hat: bfloat16 [16384, 1024], P('sp', 'tp'), may hold values from -6 to 6
- norm_rstd: float32 [16384], P('sp'), may hold values from 0.3 to 3
- norm_gain: float32 [1024], P('tp'), may hold values from 0.1 to 1.9
- out_proj: bfloat16 [2048, 1024], P(None, 'tp'), may hold values from -0.1875 to 0.1875
Outputs:
- gate_grad: bfloat16 [64, 2048, 1024], P('sp', None, 'tp')
- up_grad: bfloat16 [64, 2048, 1024], P('sp', None, 'tp')
- down_grad: bfloat16 [64, 1024, 2048], P('sp', 'tp')
- proj_grad: float32 [2048, 1024], P('sp', 'tp')
- value_grad: bfloat16 [16384, 1024], P('sp', 'tp')
- gate_in_grad: bfloat16 [16384, 1024], P('sp', 'tp')
The draws below stay inside these ranges and needn't reach their ends.
Inputs may be any that keep to these rules, and one draw needn't show every extreme that they name: In the rows of one device (aligned blocks of 256 tokens) no expert is named by more than 12 routes, and in every draw some expert is named by exactly 12 in some block; a token's two experts differ.
All inputs are finite; a program needn't handle non-finite values.
Results may differ from the reference program's by a relative error of at most 0.009.
Values may be sent and summed in bfloat16 or wider, within the bound.
No kernel may reach another device: no remote copies, remote signals or barrier semaphores. Data moves between devices by JAX's collectives and lax.ppermute only.
A program may use at most 128 MiB of HBM per device.

```python
import math
import jax
import jax.numpy as jnp
import numpy as np
from jax import lax

D = 2048
CONV = 1024
FF = 1024
KERNEL = 31
TOK_DEV = 256
EXPERTS = 64
CAP = 12
TOKENS = 16384
N_TP = 4


def raised(array, own_key, source, target, blocks, factor):
    owner, partner = [(jnp.arange(array.shape[axis_at]) // (array.shape[axis_at] // blocks)).reshape([-1 if axis == axis_at else 1 for axis in range(array.ndim)]) for axis_at in (source, target)]
    chosen = jax.random.permutation(own_key, blocks)[partner]
    strong = (owner == chosen) | (owner == (partner + blocks // 2) % blocks)
    return jnp.where(strong, factor * array, array)


def steps_of(own_key, extent, split, smallest, largest):
    level = 1.0
    for axis_at, shards_of in split:
        steps = jax.random.uniform(jax.random.fold_in(jax.random.fold_in(own_key, 6), axis_at), (shards_of,), jnp.float32, smallest / len(split), largest / len(split))
        level = level * jnp.repeat(jnp.exp(steps), extent[axis_at] // shards_of).reshape((-1,) + (1,) * (len(extent) - 1 - axis_at))
    return level


def deal_out(key, own, number, rows, number_of, top, most, lean):
    sequence = jax.random.permutation(key, number_of)
    crowded, common = shares(number_of, rows * top, most, lean, True), shares(number_of, rows * top, most, lean, False)
    places = jnp.arange(number_of)

    def named(sizes, rotation):
        used = int((sizes > 0).sum())
        fixed = max(1, used // 4)
        passed = fixed + (places - fixed + rotation * (used - fixed)) % max(1, number_of - fixed)
        return jnp.zeros((number_of,), jnp.int32).at[sequence[jnp.where(places < fixed, places, passed)]].set(jnp.asarray(sizes, jnp.int32))

    sizes = jnp.where(number % 4 == 0, named(crowded, number // 4), named(common, number - number // 4 - 1))
    mixed = jax.random.permutation(jax.random.fold_in(own, 3), number_of)
    source_of, sink = mixed[0:number_of // 2 * 2:2], mixed[1:number_of // 2 * 2:2]
    room = jnp.minimum(sizes[source_of] - 1, most - sizes[sink]) // 2
    room = jnp.where((source_of == sequence[0]) | (sink == sequence[0]) | (sizes[sink] == 0), 0, jnp.maximum(room, 0))
    passed = jax.random.randint(jax.random.fold_in(own, 4), (number_of // 2,), 0, 1 << 20) % (room + 1)
    sizes = sizes.at[source_of].add(-passed).at[sink].add(passed)
    items = jnp.searchsorted(jnp.cumsum(sizes), jnp.arange(rows * top), side="right").astype(jnp.int32)
    grid = items.reshape(top, rows).T
    grid = grid[jax.random.permutation(jax.random.fold_in(own, 1), rows)]
    rotation = jax.random.randint(jax.random.fold_in(own, 2), (rows, 1), 0, top)
    return jnp.take_along_axis(grid, (jnp.arange(top)[None, :] + rotation) % top, axis=1)


def shares(number_of, total, limit, slope, full):
    weights = [(1 << 20) // math.isqrt(grade ** slope) + 1 for grade in range(1, number_of + 1)]
    largest = limit if full else min(limit, max(-(-total // number_of), total * weights[0] // sum(weights)))
    least = 1 if total - largest >= number_of - 1 else 0
    counts, surplus = [largest] + [least] * (number_of - 1), total - largest - least * (number_of - 1)
    while surplus > 0:
        candidates = [i for i in range(1, number_of) if counts[i] < largest] or [i for i in range(1, number_of) if counts[i] < limit]
        pool, left = sum([weights[i] for i in candidates]), surplus
        for i in candidates:
            extra = min(limit - counts[i], max(1, left * weights[i] // pool), surplus)
            counts[i] = counts[i] + extra
            surplus = surplus - extra
    return np.array(counts)


def noise(stream_key, dims, spread, limit, split=(), kind=jnp.bfloat16):
    values = spread * jax.random.normal(stream_key, dims, jnp.float32)
    if split:
        values = values * steps_of(stream_key, dims, split, -0.22, 0.18)
    return jnp.clip(values, -limit, limit).astype(kind)


def gaussian_with(rng, dims, deviation, limit, shards, heavy, kind=jnp.bfloat16):
    drawn = deviation * jax.random.normal(rng, dims, jnp.float32)
    if shards:
        drawn = drawn * steps_of(rng, dims, shards, -0.22, 0.18)
    return jnp.clip(raised(drawn, jax.random.fold_in(rng, 3), *heavy), -limit, limit).astype(kind)


def setup_inputs(seed: int = 0) -> dict:
    seeds = jax.random.split(jax.random.key(seed), 16)
    moe_input = noise(seeds[0], (TOKENS, D), 1.0, 6.0, ((0, 64),))
    out_cotangent = gaussian_with(seeds[1], (TOKENS, D), 1.0, 16.0, ((0, 64),), (0, 1, 64, 4.0))
    routes_keys = jax.random.split(jax.random.fold_in(seeds[2], 1), TOKENS // TOK_DEV)
    routes_turns = jax.random.permutation(jax.random.fold_in(seeds[2], 3), TOKENS // TOK_DEV)
    routes = jax.vmap(lambda own, number: deal_out(jax.random.fold_in(seeds[2], 2), own, number, TOK_DEV, EXPERTS, 2, CAP, 2))(routes_keys, routes_turns).reshape((TOKENS, 2))
    group_weight = jnp.clip(0.5 + 0.5 * jax.random.uniform(seeds[3], (TOKENS,), jnp.float32) ** steps_of(seeds[3], (TOKENS,), ((0, 64),), -0.2, 0.2), 0.5, 1.0)
    inner_weight = jnp.clip(0.3 + 0.7 * jax.random.uniform(seeds[4], (TOKENS, 2), jnp.float32) ** steps_of(seeds[4], (TOKENS, 2), ((0, 64),), -0.2, 0.2), 0.3, 1.0)
    gate_weight = noise(seeds[5], (EXPERTS, D, FF), D ** -0.5, 0.125, ((0, 64), (2, 4)))
    up_weight = noise(seeds[6], (EXPERTS, D, FF), D ** -0.5, 0.125, ((0, 64), (2, 4)))
    down_weight = noise(seeds[7], (EXPERTS, FF, D), FF ** -0.5, 0.1875, ((0, 64), (1, 4)))
    value_in = noise(seeds[8], (TOKENS, CONV), 1.0, 6.0, ((0, 64), (1, 4)))
    gate_in = noise(seeds[9], (TOKENS, CONV), 1.0, 6.0, ((0, 64), (1, 4)))
    conv_taps = noise(seeds[10], (KERNEL, CONV), KERNEL ** -0.5, 1.0, ((1, 4),))
    norm_hat = noise(seeds[11], (TOKENS, CONV), 1.0, 6.0, ((0, 64), (1, 4)))
    norm_rstd = jnp.clip(jnp.exp(math.log(3.0) - 2.3025851 * jax.random.uniform(seeds[12], (TOKENS,), jnp.float32) ** steps_of(seeds[12], (TOKENS,), ((0, 64),), -0.2, 0.2)), 0.3, 3.0)
    norm_gain = jnp.clip(1.0 + 0.18 * jax.random.normal(seeds[13], (CONV,), jnp.float32), 0.1, 1.9)
    out_proj = noise(seeds[14], (D, CONV), CONV ** -0.5, 0.1875, ((1, 4),))
    return dict(moe_input=moe_input, out_cotangent=out_cotangent, routes=routes, group_weight=group_weight, inner_weight=inner_weight, gate_weight=gate_weight, up_weight=up_weight, down_weight=down_weight, value_in=value_in, gate_in=gate_in, conv_taps=conv_taps, norm_hat=norm_hat, norm_rstd=norm_rstd, norm_gain=norm_gain, out_proj=out_proj)


def round_half(values):
    return lax.optimization_barrier(values.astype(jnp.bfloat16)).astype(jnp.float32)


def silu_slope(logits, squashed):
    return squashed * (1.0 + logits * (1.0 - squashed))


def reference(moe_input, out_cotangent, routes, group_weight, inner_weight, gate_weight, up_weight, down_weight, value_in, gate_in, conv_taps, norm_hat, norm_rstd, norm_gain, out_proj):
    tok_total, model_width = moe_input.shape
    all_experts = gate_weight.shape[0]
    hidden_units = gate_weight.shape[2]
    block_count = tok_total // TOK_DEV
    block_routes = 2 * TOK_DEV
    total_routes = 2 * tok_total
    routes_flat = routes.reshape(block_count, block_routes).astype(jnp.int32)
    one_hot = (routes_flat[:, :, None] == jnp.arange(all_experts, dtype=jnp.int32)[None, None, :]).astype(jnp.int32)
    slot_rank = jnp.sum(one_hot * (jnp.cumsum(one_hot, axis=1) - one_hot), axis=2)
    expert_rows = block_count * CAP
    slot_index = routes_flat * expert_rows + jnp.arange(block_count, dtype=jnp.int32)[:, None] * CAP + slot_rank
    slot_index = slot_index.reshape(total_routes).astype(jnp.int32)
    slot_owner = jnp.full((all_experts * expert_rows,), total_routes, jnp.int32).at[slot_index].set(jnp.arange(total_routes, dtype=jnp.int32))
    route_weight = group_weight[:, None] * inner_weight
    scaled = (route_weight[:, :, None] * out_cotangent.astype(jnp.float32)[:, None, :]).astype(jnp.bfloat16)
    scaled = jnp.concatenate([scaled.reshape(total_routes, model_width), jnp.zeros((1, model_width), jnp.bfloat16)])
    inputs = jnp.concatenate([moe_input, jnp.zeros((1, model_width), jnp.bfloat16)])
    owners = slot_owner.reshape(all_experts, expert_rows)
    quarter = hidden_units // N_TP

    def one_expert(packed):
        w_gate, w_up, w_down, members = packed
        slot_grad = scaled[members]
        slot_input = inputs[members // 2]
        gate_pre = jnp.dot(slot_input, w_gate, preferred_element_type=jnp.float32)
        up_pre = jnp.dot(slot_input, w_up, preferred_element_type=jnp.float32)
        gate_sigma = jax.nn.sigmoid(gate_pre)
        hidden_act = (gate_pre * gate_sigma * up_pre).astype(jnp.bfloat16)
        act_grad = jnp.dot(slot_grad, w_down.T, preferred_element_type=jnp.float32)
        gate_delta = (act_grad * up_pre * silu_slope(gate_pre, gate_sigma)).astype(jnp.bfloat16)
        up_delta = (act_grad * gate_pre * gate_sigma).astype(jnp.bfloat16)
        down_part = jnp.dot(hidden_act.T, slot_grad, preferred_element_type=jnp.float32).astype(jnp.bfloat16)
        gate_part = jnp.dot(slot_input.T, gate_delta, preferred_element_type=jnp.float32).astype(jnp.bfloat16)
        up_part = jnp.dot(slot_input.T, up_delta, preferred_element_type=jnp.float32).astype(jnp.bfloat16)
        summed = jnp.zeros((members.shape[0], model_width), jnp.float32)
        for block in range(N_TP):
            lower = block * quarter
            upper = lower + quarter
            partial_value = jnp.dot(gate_delta[:, lower:upper], w_gate[:, lower:upper].T, preferred_element_type=jnp.float32)
            partial_value = partial_value + jnp.dot(up_delta[:, lower:upper], w_up[:, lower:upper].T, preferred_element_type=jnp.float32)
            summed = summed + round_half(partial_value)
        return gate_part, up_part, down_part, summed.astype(jnp.bfloat16)

    gate_grad, up_grad, down_grad, slot_back = lax.map(one_expert, (gate_weight, up_weight, down_weight, owners))
    route_back = slot_back.reshape(all_experts * expert_rows, model_width)[slot_index]
    returned = jnp.sum(route_back.reshape(tok_total, 2, model_width).astype(jnp.float32), axis=1)
    mixer_grad = (out_cotangent.astype(jnp.float32) + returned).astype(jnp.bfloat16)
    normed = norm_hat.astype(jnp.float32) * norm_gain[None, :]
    norm_sigma = jax.nn.sigmoid(normed)
    mixer_act = (normed * norm_sigma).astype(jnp.bfloat16)
    proj_grad = jnp.dot(mixer_grad.T, mixer_act, preferred_element_type=jnp.float32)
    silu_grad = jnp.dot(mixer_grad, out_proj, preferred_element_type=jnp.float32)
    hat_grad = silu_grad * silu_slope(normed, norm_sigma) * norm_gain[None, :]
    norm_values = norm_hat.astype(jnp.float32)
    grad_mean = jnp.mean(hat_grad, axis=1, keepdims=True)
    grad_dot = jnp.mean(hat_grad * norm_values, axis=1, keepdims=True)
    conv_grad = norm_rstd[:, None] * (hat_grad - grad_mean - norm_values * grad_dot)
    tap_count = conv_taps.shape[0]
    extended = jnp.pad(conv_grad, ((0, tap_count - 1), (0, 0)))
    tap_values = conv_taps.astype(jnp.float32)
    glu_grad = jnp.zeros_like(conv_grad)
    for offset in range(tap_count):
        lower = tap_count - 1 - offset
        glu_grad = glu_grad + tap_values[offset][None, :] * extended[lower:lower + tok_total]
    gate_sigma = jax.nn.sigmoid(gate_in.astype(jnp.float32))
    value_grad = (glu_grad * gate_sigma).astype(jnp.bfloat16)
    gate_in_grad = (glu_grad * value_in.astype(jnp.float32) * gate_sigma * (1.0 - gate_sigma)).astype(jnp.bfloat16)
    return gate_grad, up_grad, down_grad, proj_grad, value_grad, gate_in_grad
```

```python
import functools

import jax
import jax.numpy as jnp
import numpy as np
from jax import lax
from jax.experimental import pallas as pl
from jax.experimental.pallas import tpu as pltpu
from jax.sharding import PartitionSpec as P


BF = jnp.bfloat16
F32 = jnp.float32
TOK = 256
WIDTH = 2048
HALF = 1024
QUART = 512
CH = 256
HID = 256
EXPERTS = 64
CAP = 12
SUB = 6
ROWS = 64 * SUB
SLOTS = 64 * 24
AUX = 512 + 256 + 16
PAIR_W = [(0, 1), (1, 0), (2, 3), (3, 2)]
PAIR_R = [(0, 3), (3, 0), (1, 2), (2, 1)]

NT = (((1,), (1,)), ((), ()))
TN = (((0,), (0,)), ((), ()))


def dot(a, b):
    return jnp.dot(a, b, preferred_element_type=F32)


def dotg(a, b, dims):
    return lax.dot_general(a, b, dims, preferred_element_type=F32)


def spot():
    j = lax.axis_index("tp")
    half = lax.shift_right_logical(j, 1)
    row_class = lax.rem(lax.shift_right_logical(j + 1, 1), 2)
    return j, half, row_class


def at(start, size):
    return pl.ds(pl.multiple_of(start, 128), size)


def call(body, outs, args, flops, smem=(), mem=None):
    bytes_moved = sum(a.size * a.dtype.itemsize for a in args) + sum(
        np.prod(s) * np.dtype(d).itemsize for s, d in outs
    )
    return pl.pallas_call(
        body,
        out_shape=[jax.ShapeDtypeStruct(s, d) for s, d in outs],
        in_specs=[pl.BlockSpec(memory_space=pltpu.VMEM)] * len(args),
        out_specs=[pl.BlockSpec(memory_space=pltpu.VMEM)] * len(outs),
        cost_estimate=pl.CostEstimate(
            flops=int(flops), bytes_accessed=int(bytes_moved), transcendentals=0
        ),
        compiler_params=pltpu.CompilerParams(vmem_limit_bytes=48 * 1024 * 1024),
    )(*args)


def slot_parts(i):
    who = lax.shift_right_logical(i * 2731, 16)
    rest = i - who * 24
    part = lax.shift_right_logical(rest * 43, 8)
    return who, part, rest - part * 6


def pack_body(routes_ref, weight_ref, input_ref, grad_ref, send_ref, code_ref):
    _, half, row_class = spot()
    experts = lax.broadcasted_iota(jnp.int32, (EXPERTS, TOK), 0)
    first, second = routes_ref[0:1, :], routes_ref[1:2, :]
    is_first, is_second = experts == first, experts == second
    before = lax.broadcasted_iota(jnp.int32, (TOK, TOK), 0) < lax.broadcasted_iota(
        jnp.int32, (TOK, TOK), 1
    )
    before = jnp.where(before, 1.0, 0.0).astype(BF)
    one_first = jnp.where(is_first, 1.0, 0.0)
    one_second = jnp.where(is_second, 1.0, 0.0)
    count_first = dot(one_first.astype(BF), before)
    count_second = dot(one_second.astype(BF), before) + jnp.sum(one_first, axis=1, keepdims=True)
    rank_first = jnp.sum(one_first * count_first, axis=0, keepdims=True).astype(jnp.int32)
    rank_second = jnp.sum(one_second * count_second, axis=0, keepdims=True).astype(jnp.int32)
    code_first = first * CAP + rank_first
    code_second = second * CAP + rank_second
    codes = jnp.concatenate(
        [
            jnp.broadcast_to(code_first.astype(F32), (64, TOK)),
            jnp.broadcast_to(code_second.astype(F32), (64, TOK)),
        ],
        axis=0,
    )
    code_ref[...] = jnp.transpose(codes)
    data = jnp.concatenate(
        [
            input_ref[:, at(half * HALF, QUART)],
            input_ref[:, at(half * HALF + QUART, QUART)],
            grad_ref[:, at(half * HALF, QUART)],
            grad_ref[:, at(half * HALF + QUART, QUART)],
        ],
        axis=0,
    )
    step = 384
    who, part, rank = slot_parts(lax.broadcasted_iota(jnp.int32, (step, TOK), 0))
    base = who * CAP + rank
    w_first, w_second = weight_ref[0:1, :], weight_ref[1:2, :]
    for k in range(SLOTS // step):
        target = base + (k * (step // 24) * CAP + row_class * SUB)
        hit_first = target == code_first
        hit_second = target == code_second
        scale = jnp.sum(
            jnp.where(hit_first, w_first, 0.0) + jnp.where(hit_second, w_second, 0.0),
            axis=1,
            keepdims=True,
        )
        scale = jnp.where(part[:, 0:1] >= 2, scale, 1.0)
        pick = jnp.where(hit_first, 1.0, jnp.where(hit_second, 1.0, 0.0))
        picks = jnp.concatenate(
            [jnp.where(part == q, pick, 0.0).astype(BF) for q in range(4)], axis=1
        )
        send_ref[k * step : (k + 1) * step, :] = (dot(picks, data) * scale).astype(BF)


def unpack_body(recv_ref, perm_ref, input_ref, grad_ref):
    for group in range(8):
        rows = dot(perm_ref[...], recv_ref[group * 192 : (group + 1) * 192, :]).astype(BF)
        for q in range(2):
            to = slice(q * ROWS + group * 48, q * ROWS + (group + 1) * 48)
            input_ref[to, :] = rows[q * 48 : (q + 1) * 48]
            grad_ref[to, :] = rows[(q + 2) * 48 : (q + 3) * 48]


def whole_rows(own_ref, other_ref, half, out_ref):
    for q in range(2):
        out_ref[:, at(half * HALF + q * QUART, QUART)] = own_ref[q * ROWS : (q + 1) * ROWS, :]
        out_ref[:, at((1 - half) * HALF + q * QUART, QUART)] = other_ref[
            q * ROWS : (q + 1) * ROWS, :
        ]


def forward_body(own_ref, other_ref, wg_ref, wg2_ref, wu_ref, wu2_ref, x_ref, gate_ref, up_ref):
    _, half, _ = spot()
    whole_rows(own_ref, other_ref, half, x_ref)
    x = x_ref[...]
    gate_ref[:, :HID] = dot(x, wg_ref[...])
    gate_ref[:, HID:] = dot(x, wg2_ref[...])
    up_ref[:, :HID] = dot(x, wu_ref[...])
    up_ref[:, HID:] = dot(x, wu2_ref[...])


def partial_rows(gd, ud, gd2, ud2, wg_ref, wg2_ref, wu_ref, wu2_ref, start):
    rows = at(start, HALF)
    return (
        dotg(gd, wg_ref[rows, :], NT)
        + dotg(ud, wu_ref[rows, :], NT)
        + dotg(gd2, wg2_ref[rows, :], NT)
        + dotg(ud2, wu2_ref[rows, :], NT)
    )


def delta_body(
    own_ref, other_ref, gate_ref, up_ref, wd_ref, wd2_ref, wg_ref, wg2_ref, wu_ref, wu2_ref,
    g_ref, h_ref, h2_ref, gd_ref, gd2_ref, ud_ref, ud2_ref, send_ref,
):
    _, half, _ = spot()
    whole_rows(own_ref, other_ref, half, g_ref)
    g = g_ref[...]
    for k, (w_ref, ho, go, uo) in enumerate(
        ((wd_ref, h_ref, gd_ref, ud_ref), (wd2_ref, h2_ref, gd2_ref, ud2_ref))
    ):
        act_grad = dotg(g, w_ref[...], NT)
        gate = gate_ref[:, k * HID : (k + 1) * HID]
        up = up_ref[:, k * HID : (k + 1) * HID]
        sigma = jax.nn.sigmoid(gate)
        act = gate * sigma
        ho[...] = (act * up).astype(BF)
        go[...] = (act_grad * up * (sigma * (1.0 + gate * (1.0 - sigma)))).astype(BF)
        uo[...] = (act_grad * act).astype(BF)
    send_ref[...] = partial_rows(
        gd_ref[...], ud_ref[...], gd2_ref[...], ud2_ref[...],
        wg_ref, wg2_ref, wu_ref, wu2_ref, (1 - half) * HALF,
    ).astype(BF)


def keep_body(gd_ref, gd2_ref, ud_ref, ud2_ref, wg_ref, wg2_ref, wu_ref, wu2_ref, keep_ref):
    _, half, _ = spot()
    keep_ref[...] = partial_rows(
        gd_ref[...], ud_ref[...], gd2_ref[...], ud2_ref[...],
        wg_ref, wg2_ref, wu_ref, wu2_ref, half * HALF,
    )


def back_body(keep_ref, recv_ref, perm_ref, send_ref):
    for group in range(8):
        rows = slice(group * 48, (group + 1) * 48)
        total = (keep_ref[rows, :] + recv_ref[rows, :].astype(F32)).astype(BF)
        stacked = jnp.concatenate([total[:, q * 256 : (q + 1) * 256] for q in range(4)], axis=0)
        send_ref[group * 192 : (group + 1) * 192, :] = dot(perm_ref[...], stacked).astype(BF)


def combine_body(back_ref, code_ref, grad_ref, keep_ref, send_ref):
    j, _, row_class = spot()
    who, part, rank = slot_parts(lax.broadcasted_iota(jnp.int32, (1, SLOTS), 1))
    target = (who * CAP + rank + row_class * SUB).astype(F32)
    hit = jnp.where(
        target == code_ref[:, 0:1], 1.0, jnp.where(target == code_ref[:, 64:65], 1.0, 0.0)
    )
    kept = lax.rem(j, 2) * 2
    back = back_ref[...]
    for a in range(2):
        cols = slice(a * 256, (a + 1) * 256)
        mine = dot(jnp.where(part == kept + a, hit, 0.0).astype(BF), back)
        theirs = dot(jnp.where(part == 2 - kept + a, hit, 0.0).astype(BF), back)
        own = grad_ref[:, at(j * QUART + a * 256, 256)].astype(F32)
        keep_ref[:, cols] = own + mine
        send_ref[:, cols] = theirs.astype(BF)


def aux_body(proj_ref, hat_ref, gain_ref, *out_refs):
    j, _, _ = spot()
    gain = gain_ref[...]
    top = gain.astype(BF)
    rest = gain - top.astype(F32)
    mid = rest.astype(BF)
    low = (rest - mid.astype(F32)).astype(BF)
    row = lax.broadcasted_iota(jnp.int32, (16, CH), 0)
    gains = jnp.where(
        row == 0,
        top.astype(F32),
        jnp.where(row == 1, mid.astype(F32), jnp.where(row == 2, low.astype(F32), 0.0)),
    ).astype(BF)
    for d, out_ref in enumerate(out_refs):
        to = lax.rem(j + d, 4)
        out_ref[0:512, :] = proj_ref[pl.ds(pl.multiple_of(to * 512, 512), 512), :]
        out_ref[512:768, :] = hat_ref[...]
        out_ref[768:784, :] = gains


def channel_body(b0_ref, b1_ref, b2_ref, b3_ref, proj_ref, act_ref, slope_ref, hat_ref):
    j, _, _ = spot()
    for d, ref in enumerate((b0_ref, b1_ref, b2_ref, b3_ref)):
        cols = at(lax.rem(j + 4 - d, 4) * CH, CH)
        proj_ref[:, cols] = ref[0:512, :]
        hat = ref[512:768, :]
        gains = ref[768:784, :].astype(F32)
        gain = gains[0:1, :] + gains[1:2, :] + gains[2:3, :]
        normed = hat.astype(F32) * gain
        sigma = jax.nn.sigmoid(normed)
        hat_ref[:, cols] = hat
        act_ref[:, cols] = (normed * sigma).astype(BF)
        slope_ref[:, cols] = sigma * (1.0 + normed * (1.0 - sigma)) * gain


def mixed(keep_ref, recv_ref):
    return (keep_ref[...] + recv_ref[...].astype(F32)).astype(BF)


def outer_body(keep_ref, recv_ref, act_ref, send_ref):
    mix = mixed(keep_ref, recv_ref)
    turned = jnp.transpose(mix.astype(F32)).astype(BF)
    for k in range(4):
        send_ref[k * 512 : (k + 1) * 512, :] = dot(
            turned, act_ref[:, k * CH : (k + 1) * CH]
        ).astype(BF)


def silu_body(keep_ref, recv_ref, proj_ref, slope_ref, hat_ref, send_ref):
    mix = mixed(keep_ref, recv_ref)
    part = dot(mix, proj_ref[...])
    sloped = part * slope_ref[...]
    dotted = sloped * hat_ref[...].astype(F32)
    ones = jnp.ones((16, 4 * CH), BF)
    total = dotg(ones, sloped.astype(BF), NT)
    total_dot = dotg(ones, dotted.astype(BF), NT)
    row = lax.broadcasted_iota(jnp.int32, (16, TOK), 0)
    top, top_dot = total.astype(BF).astype(F32), total_dot.astype(BF).astype(F32)
    sums = jnp.where(
        row == 0,
        top,
        jnp.where(
            row == 1,
            total - top,
            jnp.where(row == 2, top_dot, jnp.where(row == 3, total_dot - top_dot, 0.0)),
        ),
    ).astype(BF)
    for k in range(4):
        send_ref[k, 0:256, :] = part[:, k * CH : (k + 1) * CH].astype(BF)
        send_ref[k, 256:272, :] = sums


def conv_body(recv_ref, slope_ref, hat_ref, rstd_ref, out_ref):
    j, _, _ = spot()
    total = recv_ref[0, 0:256, :].astype(F32)
    for k in range(1, 4):
        total = total + recv_ref[k, 0:256, :].astype(F32)
    rows = jnp.concatenate([recv_ref[k, 256:272, :] for k in range(4)], axis=0)
    kind = lax.rem(lax.broadcasted_iota(jnp.int32, (64, CH), 0), 16)
    pick = jnp.where(kind < 2, 1.0, 0.0).astype(BF)
    pick_dot = jnp.where(kind < 2, 0.0, jnp.where(kind < 4, 1.0, 0.0)).astype(BF)
    mean = dotg(rows, pick, TN) * (1.0 / (4 * CH))
    mean_dot = dotg(rows, pick_dot, TN) * (1.0 / (4 * CH))
    hat_grad = total * slope_ref[:, at(j * CH, CH)]
    out_ref[...] = rstd_ref[...] * (hat_grad - mean - hat_ref[...].astype(F32) * mean_dot)


def unmix_matrix():
    m = np.zeros((192, 192), np.float32)
    for q in range(4):
        for s in range(8):
            for r in range(6):
                m[q * 48 + s * 6 + r, s * 24 + q * 6 + r] = 1.0
    return m


def on_device(
    moe_input,
    out_cotangent,
    routes,
    group_weight,
    inner_weight,
    gate_weight,
    up_weight,
    down_weight,
    value_in,
    gate_in,
    conv_taps,
    norm_hat,
    norm_rstd,
    norm_gain,
    out_proj,
):
    sp_count = lax.axis_size("sp")
    unmix = unmix_matrix()
    unmix_to = jnp.asarray(unmix, BF)
    unmix_from = jnp.asarray(unmix.T, BF)
    wg, wu, wd = gate_weight[0], up_weight[0], down_weight[0]
    wg2 = lax.ppermute(wg, "tp", PAIR_W)
    wu2 = lax.ppermute(wu, "tp", PAIR_W)
    wd2 = lax.ppermute(wd, "tp", PAIR_W)

    route_weight = group_weight[None, :] * inner_weight.T
    send, codes = call(
        pack_body,
        [((SLOTS, 512), BF), ((TOK, 128), F32)],
        (routes.T, route_weight, moe_input, out_cotangent),
        2 * SLOTS * 1024 * 512,
    )
    recv = lax.all_to_all(
        send.reshape(sp_count, 24, 512), "sp", split_axis=0, concat_axis=0, tiled=True
    )
    x_own, g_own = call(
        unpack_body,
        [((2 * ROWS, 512), BF)] * 2,
        (recv.reshape(SLOTS, 512), unmix_to),
        2 * SLOTS * 192 * 512,
    )
    x_other = lax.ppermute(x_own, "tp", PAIR_R)
    g_other = lax.ppermute(g_own, "tp", PAIR_R)
    x, gate_pre, up_pre = call(
        forward_body,
        [((ROWS, WIDTH), BF), ((ROWS, 2 * HID), F32), ((ROWS, 2 * HID), F32)],
        (x_own, x_other, wg, wg2, wu, wu2),
        2 * ROWS * WIDTH * 4 * HID,
    )
    small = ((ROWS, HID), BF)
    g, h, h2, gd, gd2, ud, ud2, rows_send = call(
        delta_body,
        [((ROWS, WIDTH), BF), small, small, small, small, small, small, ((ROWS, HALF), BF)],
        (g_own, g_other, gate_pre, up_pre, wd, wd2, wg, wg2, wu, wu2),
        2 * ROWS * WIDTH * 4 * HID,
    )
    rows_recv = lax.ppermute(rows_send, "tp", PAIR_R)
    (rows_keep,) = call(
        keep_body,
        [((ROWS, HALF), F32)],
        (gd, gd2, ud, ud2, wg, wg2, wu, wu2),
        2 * ROWS * HALF * 4 * HID,
    )

    def outer(a, b):
        return lax.dot_general(a, b, TN, preferred_element_type=F32)

    grads = [outer(x, gd), outer(x, ud), outer(h, g)]
    grads_other = [
        lax.ppermute(v.astype(BF), "tp", PAIR_W)
        for v in (outer(x, gd2), outer(x, ud2), outer(h2, g))
    ]
    gate_grad, up_grad, down_grad = (
        (a + b.astype(F32)).astype(BF)[None] for a, b in zip(grads, grads_other)
    )

    (back_send,) = call(
        back_body,
        [((SLOTS, 256), BF)],
        (rows_keep, rows_recv, unmix_from),
        2 * SLOTS * 192 * 256,
    )
    back = lax.all_to_all(
        back_send.reshape(sp_count, 24, 256), "sp", split_axis=0, concat_axis=0, tiled=True
    )

    late = lax.optimization_barrier((out_proj, norm_hat, g_other))
    blocks = call(
        aux_body,
        [((AUX, CH), BF)] * 4,
        (late[0], late[1], norm_gain[None, :]),
        0,
    )
    blocks = [blocks[0]] + [
        lax.ppermute(blocks[d], "tp", [(i, (i + d) % 4) for i in range(4)]) for d in (1, 2, 3)
    ]
    proj_rows, act, slope, hat = call(
        channel_body,
        [((512, 4 * CH), BF), ((TOK, 4 * CH), BF), ((TOK, 4 * CH), F32), ((TOK, 4 * CH), BF)],
        blocks,
        0,
    )

    mix_keep, mix_send = call(
        combine_body,
        [((TOK, QUART), F32), ((TOK, QUART), BF)],
        (back.reshape(SLOTS, 256), codes, out_cotangent),
        2 * SLOTS * 1024 * 256,
    )
    mix_recv = lax.ppermute(mix_send, "tp", PAIR_W)
    (outer_send,) = call(
        outer_body,
        [((2048, CH), BF)],
        (mix_keep, mix_recv, act),
        2 * TOK * 512 * 1024,
    )
    outer_recv = lax.all_to_all(
        outer_send.reshape(sp_count, 2048 // sp_count, CH),
        "sp",
        split_axis=0,
        concat_axis=0,
        tiled=True,
    )
    piece = jnp.sum(outer_recv.astype(F32), axis=0)
    per_tp = sp_count // 4
    proj_grad = lax.ppermute(
        piece,
        ("sp", "tp"),
        [
            (s * 4 + t, (per_tp * t + s % per_tp) * 4 + s // per_tp)
            for s in range(sp_count)
            for t in range(4)
        ],
    )

    (silu_send,) = call(
        silu_body,
        [((4, 272, CH), BF)],
        (mix_keep, mix_recv, proj_rows, slope, hat),
        2 * TOK * 512 * 1024,
    )
    silu_recv = lax.all_to_all(silu_send, "tp", split_axis=0, concat_axis=0, tiled=True)
    (conv_grad,) = call(
        conv_body,
        [((TOK, CH), F32)],
        (silu_recv, slope, norm_hat, norm_rstd[:, None]),
        0,
    )
    tap_count = conv_taps.shape[0]
    incoming = lax.ppermute(
        conv_grad[: tap_count - 1], "sp", [(i, i - 1) for i in range(1, sp_count)]
    )
    extended = jnp.concatenate([conv_grad, incoming], axis=0)
    tap_values = conv_taps.astype(F32)
    glu_grad = jnp.zeros_like(conv_grad)
    for offset in range(tap_count):
        lower = tap_count - 1 - offset
        glu_grad = glu_grad + tap_values[offset][None, :] * extended[lower : lower + TOK]
    input_sigma = jax.nn.sigmoid(gate_in.astype(F32))
    value_grad = (glu_grad * input_sigma).astype(BF)
    gate_in_grad = (
        glu_grad * value_in.astype(F32) * input_sigma * (1.0 - input_sigma)
    ).astype(BF)
    return (gate_grad, up_grad, down_grad, proj_grad, value_grad, gate_in_grad)


def solution(mesh):
    return jax.shard_map(
        on_device,
        mesh=mesh,
        in_specs=(
            P("sp", None),
            P("sp", None),
            P("sp", None),
            P("sp"),
            P("sp", None),
            P("sp", None, "tp"),
            P("sp", None, "tp"),
            P("sp", "tp", None),
            P("sp", "tp"),
            P("sp", "tp"),
            P(None, "tp"),
            P("sp", "tp"),
            P("sp"),
            P("tp"),
            P(None, "tp"),
        ),
        out_specs=(
            P("sp", None, "tp"),
            P("sp", None, "tp"),
            P("sp", "tp", None),
            P("sp", "tp"),
            P("sp", "tp"),
            P("sp", "tp"),
        ),
        check_vma=False,
    )
```

```python
import jax
import jax.numpy as jnp
import numpy as np
from jax import lax
from jax.experimental import pallas as pl
from jax.experimental.pallas import tpu as pltpu
from jax.sharding import PartitionSpec as P


BF = jnp.bfloat16
F32 = jnp.float32
TOK = 256
WIDTH = 2048
HALF = 1024
QUART = 512
CH = 256
HID = 256
EXPERTS = 64
CAP = 12
SUB = 6
ROWS = 64 * SUB
SLOTS = 64 * 24
AUX = 512 + 256 + 16
VMEM_SMALL = 16 * 1024 * 1024
VMEM_LARGE = 24 * 1024 * 1024
VMEM_WHOLE = 60 * 1024 * 1024
PAIR_W = [(0, 1), (1, 0), (2, 3), (3, 2)]
PAIR_R = [(0, 3), (3, 0), (1, 2), (2, 1)]

NT = (((1,), (1,)), ((), ()))
TN = (((0,), (0,)), ((), ()))


def dot(a, b):
    return jnp.dot(a, b, preferred_element_type=F32)


def dotg(a, b, dims):
    return lax.dot_general(a, b, dims, preferred_element_type=F32)


def spot():
    j = lax.axis_index("tp")
    half = lax.shift_right_logical(j, 1)
    row_class = lax.rem(lax.shift_right_logical(j + 1, 1), 2)
    return j, half, row_class


def at(start, size):
    return pl.ds(pl.multiple_of(start, 128), size)


def call(body, outs, args, flops, in_place=(), scratch=(), vmem=VMEM_SMALL):
    bytes_moved = sum(a.size * a.dtype.itemsize for a in args) + sum(
        np.prod(s) * np.dtype(d).itemsize for s, d in outs
    )
    return pl.pallas_call(
        body,
        out_shape=[jax.ShapeDtypeStruct(s, d) for s, d in outs],
        in_specs=[
            pl.BlockSpec(memory_space=pltpu.HBM if i in in_place else pltpu.VMEM)
            for i in range(len(args))
        ],
        out_specs=[pl.BlockSpec(memory_space=pltpu.VMEM)] * len(outs),
        scratch_shapes=list(scratch),
        cost_estimate=pl.CostEstimate(
            flops=int(flops), bytes_accessed=int(bytes_moved), transcendentals=0
        ),
        compiler_params=pltpu.CompilerParams(vmem_limit_bytes=vmem),
    )(*args)


def slot_parts(i):
    who = lax.shift_right_logical(i * 2731, 16)
    rest = i - who * 24
    part = lax.shift_right_logical(rest * 43, 8)
    return who, part, rest - part * 6


def half_copy(from_ref, to_ref, sem, half):
    return pltpu.make_async_copy(from_ref.at[:, at(half * HALF, HALF)], to_ref, sem)


def pick_rows(code_first, code_second, row_class, data, send_ref, weights=None):
    step = 384
    who, part, rank = slot_parts(lax.broadcasted_iota(jnp.int32, (step, TOK), 0))
    base = who * CAP + rank
    for k in range(SLOTS // step):
        target = base + (k * (step // 24) * CAP + row_class * SUB)
        hit_first = target == code_first
        hit_second = target == code_second
        pick = jnp.where(hit_first, 1.0, jnp.where(hit_second, 1.0, 0.0))
        picks = jnp.concatenate(
            [jnp.where(part == q, pick, 0.0).astype(BF) for q in range(4)], axis=1
        )
        rows = dot(picks, data)
        if weights is not None:
            rows = rows * jnp.sum(
                jnp.where(hit_first, weights[0:1, :], 0.0)
                + jnp.where(hit_second, weights[1:2, :], 0.0),
                axis=1,
                keepdims=True,
            )
        send_ref[k * step : (k + 1) * step, :] = rows.astype(BF)


def stacked_quarters(buffer):
    return jnp.concatenate([buffer[:, q * 256 : (q + 1) * 256] for q in range(4)], axis=0)


def pack_input_body(routes_ref, input_ref, send_ref, row_ref, buffer, sem):
    _, half, row_class = spot()
    copy = half_copy(input_ref, buffer, sem, half)
    copy.start()
    experts = lax.broadcasted_iota(jnp.int32, (EXPERTS, TOK), 0)
    first, second = routes_ref[0:1, :], routes_ref[1:2, :]
    before = lax.broadcasted_iota(jnp.int32, (TOK, TOK), 0) < lax.broadcasted_iota(
        jnp.int32, (TOK, TOK), 1
    )
    before = jnp.where(before, 1.0, 0.0).astype(BF)
    one_first = jnp.where(experts == first, 1.0, 0.0)
    one_second = jnp.where(experts == second, 1.0, 0.0)
    count_first = dot(one_first.astype(BF), before)
    count_second = dot(one_second.astype(BF), before) + jnp.sum(one_first, axis=1, keepdims=True)
    rank_first = jnp.sum(one_first * count_first, axis=0, keepdims=True).astype(jnp.int32)
    rank_second = jnp.sum(one_second * count_second, axis=0, keepdims=True).astype(jnp.int32)
    code_first = first * CAP + rank_first
    code_second = second * CAP + rank_second
    row_ref[0:1, :] = code_first
    row_ref[1:2, :] = code_second
    copy.wait()
    pick_rows(code_first, code_second, row_class, stacked_quarters(buffer[...]), send_ref)


def pack_grad_body(row_ref, weight_ref, grad_ref, send_ref, code_ref, cols_ref, buffer, sem):
    j, half, row_class = spot()
    copy = half_copy(grad_ref, buffer, sem, half)
    copy.start()
    code_first, code_second = row_ref[0:1, :], row_ref[1:2, :]
    codes = jnp.concatenate(
        [
            jnp.broadcast_to(code_first.astype(F32), (64, TOK)),
            jnp.broadcast_to(code_second.astype(F32), (64, TOK)),
        ],
        axis=0,
    )
    code_ref[...] = jnp.transpose(codes)
    copy.wait()
    cols_ref[...] = buffer[:, at(lax.rem(j, 2) * QUART, QUART)]
    pick_rows(
        code_first,
        code_second,
        row_class,
        stacked_quarters(buffer[...]),
        send_ref,
        weight_ref[...],
    )


def unpack_body(recv_ref, perm_ref, out_ref):
    for group in range(8):
        rows = dot(perm_ref[...], recv_ref[group * 192 : (group + 1) * 192, :]).astype(BF)
        for q in range(4):
            out_ref[group * 48 : (group + 1) * 48, q * 256 : (q + 1) * 256] = rows[
                q * 48 : (q + 1) * 48
            ]


def whole_rows(own_ref, other_ref, half, out_ref):
    out_ref[:, at(half * HALF, HALF)] = own_ref[...]
    out_ref[:, at((1 - half) * HALF, HALF)] = other_ref[...]


def forward_body(own_ref, other_ref, wg_ref, wg2_ref, wu_ref, wu2_ref, x_ref, gate_ref, up_ref):
    _, half, _ = spot()
    whole_rows(own_ref, other_ref, half, x_ref)
    x = x_ref[...]
    gate_ref[:, :HID] = dot(x, wg_ref[...])
    gate_ref[:, HID:] = dot(x, wg2_ref[...])
    up_ref[:, :HID] = dot(x, wu_ref[...])
    up_ref[:, HID:] = dot(x, wu2_ref[...])


def partial_rows(gd, ud, gd2, ud2, wg_ref, wg2_ref, wu_ref, wu2_ref, start):
    rows = at(start, HALF)
    return (
        dotg(gd, wg_ref[rows, :], NT)
        + dotg(ud, wu_ref[rows, :], NT)
        + dotg(gd2, wg2_ref[rows, :], NT)
        + dotg(ud2, wu2_ref[rows, :], NT)
    )


def delta_body(
    own_ref, other_ref, gate_ref, up_ref, wd_ref, wd2_ref, wg_ref, wg2_ref, wu_ref, wu2_ref,
    g_ref, h_ref, h2_ref, gd_ref, gd2_ref, ud_ref, ud2_ref, send_ref,
):
    _, half, _ = spot()
    whole_rows(own_ref, other_ref, half, g_ref)
    g = g_ref[...]
    for k, (w_ref, ho, go, uo) in enumerate(
        ((wd_ref, h_ref, gd_ref, ud_ref), (wd2_ref, h2_ref, gd2_ref, ud2_ref))
    ):
        act_grad = dotg(g, w_ref[...], NT)
        gate = gate_ref[:, k * HID : (k + 1) * HID]
        up = up_ref[:, k * HID : (k + 1) * HID]
        sigma = jax.nn.sigmoid(gate)
        act = gate * sigma
        ho[...] = (act * up).astype(BF)
        go[...] = (act_grad * up * (sigma * (1.0 + gate * (1.0 - sigma)))).astype(BF)
        uo[...] = (act_grad * act).astype(BF)
    send_ref[...] = partial_rows(
        gd_ref[...], ud_ref[...], gd2_ref[...], ud2_ref[...],
        wg_ref, wg2_ref, wu_ref, wu2_ref, (1 - half) * HALF,
    ).astype(BF)


def keep_body(gd_ref, gd2_ref, ud_ref, ud2_ref, wg_ref, wg2_ref, wu_ref, wu2_ref, keep_ref):
    _, half, _ = spot()
    keep_ref[...] = partial_rows(
        gd_ref[...], ud_ref[...], gd2_ref[...], ud2_ref[...],
        wg_ref, wg2_ref, wu_ref, wu2_ref, half * HALF,
    )


def back_body(keep_ref, recv_ref, perm_ref, send_ref):
    for group in range(8):
        rows = slice(group * 48, (group + 1) * 48)
        total = (keep_ref[rows, :] + recv_ref[rows, :].astype(F32)).astype(BF)
        stacked = jnp.concatenate([total[:, q * 256 : (q + 1) * 256] for q in range(4)], axis=0)
        send_ref[group * 192 : (group + 1) * 192, :] = dot(perm_ref[...], stacked).astype(BF)


def combine_body(back_ref, code_ref, grad_ref, keep_ref, send_ref):
    j, _, row_class = spot()
    who, part, rank = slot_parts(lax.broadcasted_iota(jnp.int32, (1, SLOTS), 1))
    target = (who * CAP + rank + row_class * SUB).astype(F32)
    hit = jnp.where(
        target == code_ref[:, 0:1], 1.0, jnp.where(target == code_ref[:, 64:65], 1.0, 0.0)
    )
    kept = lax.rem(j, 2) * 2
    back = back_ref[...]
    for a in range(2):
        theirs = dot(jnp.where(part == 2 - kept + a, hit, 0.0).astype(BF), back)
        send_ref[:, a * 256 : (a + 1) * 256] = theirs.astype(BF)
    for a in range(2):
        cols = slice(a * 256, (a + 1) * 256)
        mine = dot(jnp.where(part == kept + a, hit, 0.0).astype(BF), back)
        keep_ref[:, cols] = grad_ref[:, cols].astype(F32) + mine


def aux_body(proj_ref, hat_ref, gain_ref, *out_refs):
    j, _, _ = spot()
    gain = gain_ref[...]
    top = gain.astype(BF)
    rest = gain - top.astype(F32)
    mid = rest.astype(BF)
    low = (rest - mid.astype(F32)).astype(BF)
    row = lax.broadcasted_iota(jnp.int32, (16, CH), 0)
    gains = jnp.where(
        row == 0,
        top.astype(F32),
        jnp.where(row == 1, mid.astype(F32), jnp.where(row == 2, low.astype(F32), 0.0)),
    ).astype(BF)
    for d, out_ref in enumerate(out_refs):
        to = lax.rem(j + d, 4)
        out_ref[0:512, :] = proj_ref[pl.ds(pl.multiple_of(to * 512, 512), 512), :]
        out_ref[512:768, :] = hat_ref[...]
        out_ref[768:784, :] = gains


def channel_body(
    b0_ref, b1_ref, b3_ref, b2_ref, row_ref, proj_ref, act_ref, slope_ref, hat_ref, rstd_ref
):
    rstd_ref[...] = jnp.transpose(jnp.broadcast_to(row_ref[...], (128, TOK)))
    j, _, _ = spot()
    for d, ref in zip((0, 1, 3, 2), (b0_ref, b1_ref, b3_ref, b2_ref)):
        cols = at(lax.rem(j + 4 - d, 4) * CH, CH)
        proj_ref[:, cols] = ref[0:512, :]
        hat = ref[512:768, :]
        gains = ref[768:784, :].astype(F32)
        gain = gains[0:1, :] + gains[1:2, :] + gains[2:3, :]
        normed = hat.astype(F32) * gain
        sigma = jax.nn.sigmoid(normed)
        hat_ref[:, cols] = hat
        act_ref[:, cols] = (normed * sigma).astype(BF)
        slope_ref[:, cols] = sigma * (1.0 + normed * (1.0 - sigma)) * gain


def mixed(keep_ref, recv_ref):
    return (keep_ref[...] + recv_ref[...].astype(F32)).astype(BF)


def outer_body(keep_ref, recv_ref, act_ref, own_ref, other_ref, turned_ref):
    mix = mixed(keep_ref, recv_ref)
    turned_ref[...] = jnp.transpose(mix.astype(F32))
    core = lax.rem(lax.axis_index("sp"), 2)

    def rows_of(parity):
        return jnp.concatenate(
            [
                turned_ref[pl.ds(pl.multiple_of((2 * b + parity) * 32, 32), 32), :]
                for b in range(8)
            ],
            axis=0,
        ).astype(BF)

    theirs, mine = rows_of(1 - core), rows_of(core)
    for k in range(4):
        act = act_ref[:, k * CH : (k + 1) * CH]
        other_ref[k * 256 : (k + 1) * 256, :] = dot(theirs, act).astype(BF)
        own_ref[k * 256 : (k + 1) * 256, :] = dot(mine, act)


def sum_body(own_ref, recv_ref, out_ref):
    out_ref[...] = (own_ref[...] + recv_ref[...].astype(F32)).astype(BF)


def silu_body(keep_ref, recv_ref, proj_ref, slope_ref, hat_ref, *refs):
    j, _, _ = spot()
    out_refs, part_ref = refs[:4], refs[4]
    mix = mixed(keep_ref, recv_ref)
    part = dot(mix, proj_ref[...])
    sloped = part * slope_ref[...]
    dotted = sloped * hat_ref[...].astype(F32)
    ones = jnp.ones((16, 4 * CH), BF)
    total = dotg(ones, sloped.astype(BF), NT)
    total_dot = dotg(ones, dotted.astype(BF), NT)
    row = lax.broadcasted_iota(jnp.int32, (16, TOK), 0)
    top, top_dot = total.astype(BF).astype(F32), total_dot.astype(BF).astype(F32)
    sums = jnp.where(
        row == 0,
        top,
        jnp.where(
            row == 1,
            total - top,
            jnp.where(row == 2, top_dot, jnp.where(row == 3, total_dot - top_dot, 0.0)),
        ),
    ).astype(BF)
    part_ref[...] = part
    for d, out_ref in enumerate(out_refs):
        out_ref[0:256, :] = part_ref[:, at(lax.rem(j + d, 4) * CH, CH)].astype(BF)
        out_ref[256:272, :] = sums


def conv_body(r0_ref, r1_ref, r2_ref, r3_ref, slope_ref, hat_ref, rstd_ref, out_ref, head_ref):
    j, _, _ = spot()
    recv_refs = (r0_ref, r1_ref, r2_ref, r3_ref)
    total = sum(ref[0:256, :].astype(F32) for ref in recv_refs)
    rows = jnp.concatenate([ref[256:272, :] for ref in recv_refs], axis=0)
    kind = lax.rem(lax.broadcasted_iota(jnp.int32, (64, CH), 0), 16)
    pick = jnp.where(kind < 2, 1.0, 0.0).astype(BF)
    pick_dot = jnp.where(kind < 2, 0.0, jnp.where(kind < 4, 1.0, 0.0)).astype(BF)
    mean = dotg(rows, pick, TN) * (1.0 / (4 * CH))
    mean_dot = dotg(rows, pick_dot, TN) * (1.0 / (4 * CH))
    hat_grad = total * slope_ref[:, at(j * CH, CH)]
    out_ref[...] = rstd_ref[:, 0:1] * (hat_grad - mean - hat_ref[...].astype(F32) * mean_dot)
    head_ref[...] = out_ref[0:32, :]


def taps_body(grad_ref, next_ref, taps_ref, gate_ref, value_ref, out_ref, gate_out_ref, long_ref):
    long_ref[0:256, :] = grad_ref[...]
    long_ref[256:288, :] = next_ref[...]
    for block in range(4):
        row = block * 64
        total = jnp.zeros((64, CH), F32)
        for k in range(31):
            tap = taps_ref[k : k + 1, :].astype(F32)
            total = total + tap * long_ref[row + 30 - k : row + 94 - k, :]
        rows = slice(row, row + 64)
        sigma = jax.nn.sigmoid(gate_ref[rows, :].astype(F32))
        out_ref[rows, :] = (total * sigma).astype(BF)
        gate_out_ref[rows, :] = (
            total * value_ref[rows, :].astype(F32) * sigma * (1.0 - sigma)
        ).astype(BF)


def around(blocks):
    return [lax.ppermute(blocks[d], "tp", [(i, (i + d) % 4) for i in range(4)]) for d in (1, 3, 2)]


def exchanged(array, **groups):
    return lax.all_to_all(array, "sp", split_axis=0, concat_axis=0, tiled=True, **groups)


def unmix_matrix():
    m = np.zeros((192, 192), np.float32)
    for q in range(4):
        for s in range(8):
            for r in range(6):
                m[q * 48 + s * 6 + r, s * 24 + q * 6 + r] = 1.0
    return m


def on_device(
    moe_input,
    out_cotangent,
    routes,
    group_weight,
    inner_weight,
    gate_weight,
    up_weight,
    down_weight,
    value_in,
    gate_in,
    conv_taps,
    norm_hat,
    norm_rstd,
    norm_gain,
    out_proj,
):
    sp_count = lax.axis_size("sp")
    unmix = unmix_matrix()
    unmix_to = jnp.asarray(unmix, BF)
    unmix_from = jnp.asarray(unmix.T, BF)
    wg, wu, wd = gate_weight[0], up_weight[0], down_weight[0]
    wg2 = lax.ppermute(wg, "tp", PAIR_W)
    wu2 = lax.ppermute(wu, "tp", PAIR_W)
    wd2 = lax.ppermute(wd, "tp", PAIR_W)

    route_weight = group_weight[None, :] * inner_weight.T
    buffer = [pltpu.VMEM((TOK, HALF), BF), pltpu.SemaphoreType.DMA]
    x_send, code_rows = call(
        pack_input_body,
        [((SLOTS, 256), BF), ((2, TOK), jnp.int32)],
        (routes.T, moe_input),
        2 * SLOTS * 1024 * 256,
        vmem=VMEM_WHOLE,
        in_place=(1,),
        scratch=buffer,
    )
    g_send, codes, own_cols = call(
        pack_grad_body,
        [((SLOTS, 256), BF), ((TOK, 128), F32), ((TOK, QUART), BF)],
        (code_rows, route_weight, out_cotangent),
        2 * SLOTS * 1024 * 256,
        in_place=(2,),
        scratch=buffer,
    )

    blocks = call(
        aux_body,
        [((AUX, CH), BF)] * 4,
        (out_proj, norm_hat, norm_gain[None, :]),
        0,
    )
    blocks = [blocks[0]] + around(blocks)
    proj_rows, act, slope, hat, rstd = call(
        channel_body,
        [((512, 4 * CH), BF), ((TOK, 4 * CH), BF), ((TOK, 4 * CH), F32), ((TOK, 4 * CH), BF), ((TOK, 128), F32)],
        (*blocks, norm_rstd[None, :]),
        0,
    )

    def dispatched(send):
        recv = exchanged(send.reshape(sp_count, 24, 256))
        (own,) = call(
            unpack_body,
            [((ROWS, HALF), BF)],
            (recv.reshape(SLOTS, 256), unmix_to),
            2 * SLOTS * 192 * 256,
        )
        return own, lax.ppermute(own, "tp", PAIR_R)

    x_own, x_other = dispatched(x_send)
    g_own, g_other = dispatched(g_send)
    x, gate_pre, up_pre = call(
        forward_body,
        [((ROWS, WIDTH), BF), ((ROWS, 2 * HID), F32), ((ROWS, 2 * HID), F32)],
        (x_own, x_other, wg, wg2, wu, wu2),
        2 * ROWS * WIDTH * 4 * HID,
        vmem=VMEM_LARGE,
    )
    small = ((ROWS, HID), BF)
    g, h, h2, gd, gd2, ud, ud2, rows_send = call(
        delta_body,
        [((ROWS, WIDTH), BF), small, small, small, small, small, small, ((ROWS, HALF), BF)],
        (g_own, g_other, gate_pre, up_pre, wd, wd2, wg, wg2, wu, wu2),
        2 * ROWS * WIDTH * 4 * HID,
        vmem=VMEM_LARGE,
    )
    rows_recv = lax.ppermute(rows_send, "tp", PAIR_R)
    (rows_keep,) = call(
        keep_body,
        [((ROWS, HALF), F32)],
        (gd, gd2, ud, ud2, wg, wg2, wu, wu2),
        2 * ROWS * HALF * 4 * HID,
        vmem=VMEM_LARGE,
    )

    def outer(a, b):
        return lax.dot_general(a, b, TN, preferred_element_type=F32)

    def finished(a, b, b_other):
        other = outer(*b_other).astype(BF)
        arrived = lax.ppermute(other, "tp", PAIR_W)
        return (outer(a, b) + arrived.astype(F32)).astype(BF)[None]

    gate_grad = finished(x, gd, (x, gd2))
    up_grad = finished(x, ud, (x, ud2))
    down_grad = finished(h, g, (h2, g))

    (back_send,) = call(
        back_body,
        [((SLOTS, 256), BF)],
        (rows_keep, rows_recv, unmix_from),
        2 * SLOTS * 192 * 256,
    )
    back = exchanged(back_send.reshape(sp_count, 24, 256))

    mix_keep, mix_send = call(
        combine_body,
        [((TOK, QUART), F32), ((TOK, QUART), BF)],
        (back.reshape(SLOTS, 256), codes, own_cols),
        2 * SLOTS * 1024 * 256,
    )
    mix_recv = lax.ppermute(mix_send, "tp", PAIR_W)
    outer_own, outer_other = call(
        outer_body,
        [((1024, CH), F32), ((1024, CH), BF)],
        (mix_keep, mix_recv, act),
        2 * TOK * 512 * 1024,
        scratch=[pltpu.VMEM((512, TOK), F32)],
    )
    outer_recv = lax.ppermute(outer_other, "sp", [(i, i ^ 1) for i in range(sp_count)])
    (outer_sum,) = call(sum_body, [((1024, CH), BF)], (outer_own, outer_recv), 0)
    pieces = exchanged(
        outer_sum.reshape(sp_count // 2, 32, CH),
        axis_index_groups=[list(range(c, sp_count, 2)) for c in range(2)],
    )
    piece = jnp.sum(pieces.astype(F32), axis=0)
    per_tp = sp_count // 4
    proj_grad = lax.ppermute(
        piece,
        ("sp", "tp"),
        [
            (s * 4 + t, (per_tp * t + s % per_tp) * 4 + s // per_tp)
            for s in range(sp_count)
            for t in range(4)
        ],
    )

    silu_parts = call(
        silu_body,
        [((272, CH), BF)] * 4,
        (mix_keep, mix_recv, proj_rows, slope, hat),
        2 * TOK * 512 * 1024,
        scratch=[pltpu.VMEM((TOK, 4 * CH), F32)],
    )
    silu_parts = [silu_parts[0]] + around(silu_parts)
    conv_grad, head = call(
        conv_body,
        [((TOK, CH), F32), ((32, CH), F32)],
        (*silu_parts, slope, norm_hat, rstd),
        0,
    )
    incoming = lax.ppermute(head, "sp", [(i, i - 1) for i in range(1, sp_count)])
    value_grad, gate_in_grad = call(
        taps_body,
        [((TOK, CH), BF), ((TOK, CH), BF)],
        (conv_grad, incoming, conv_taps, gate_in, value_in),
        0,
        scratch=[pltpu.VMEM((TOK + 32, CH), F32)],
    )
    return (gate_grad, up_grad, down_grad, proj_grad, value_grad, gate_in_grad)


def solution(mesh):
    return jax.shard_map(
        on_device,
        mesh=mesh,
        in_specs=(
            P("sp", None),
            P("sp", None),
            P("sp", None),
            P("sp"),
            P("sp", None),
            P("sp", None, "tp"),
            P("sp", None, "tp"),
            P("sp", "tp", None),
            P("sp", "tp"),
            P("sp", "tp"),
            P(None, "tp"),
            P("sp", "tp"),
            P("sp"),
            P("tp"),
            P(None, "tp"),
        ),
        out_specs=(
            P("sp", None, "tp"),
            P("sp", None, "tp"),
            P("sp", "tp", None),
            P("sp", "tp"),
            P("sp", "tp"),
            P("sp", "tp"),
        ),
        check_vma=False,
    )
```

```python
import jax
import jax.numpy as jnp
import numpy as np
from jax import lax
from jax.experimental import pallas as pl
from jax.experimental.pallas import tpu as pltpu
from jax.sharding import PartitionSpec as P


BF = jnp.bfloat16
F32 = jnp.float32
TOK = 256
WIDTH = 2048
HALF = 1024
QUART = 512
CH = 256
HID = 256
EXPERTS = 64
CAP = 12
SUB = 6
ROWS = 64 * SUB
PART = ROWS // 2
SLOTS = 64 * 24
AUX = 512 + 256 + 16
VMEM_SMALL = 16 * 1024 * 1024
VMEM_LARGE = 24 * 1024 * 1024
VMEM_WHOLE = 60 * 1024 * 1024
PAIR_W = [(0, 1), (1, 0), (2, 3), (3, 2)]
PAIR_R = [(0, 3), (3, 0), (1, 2), (2, 1)]

NT = (((1,), (1,)), ((), ()))
TN = (((0,), (0,)), ((), ()))


def dot(a, b):
    return jnp.dot(a, b, preferred_element_type=F32)


def dotg(a, b, dims):
    return lax.dot_general(a, b, dims, preferred_element_type=F32)


def spot():
    j = lax.axis_index("tp")
    half = lax.shift_right_logical(j, 1)
    row_class = lax.rem(lax.shift_right_logical(j + 1, 1), 2)
    return j, half, row_class


def peers(j):
    return 3 - j, j + 1 - 2 * lax.rem(j, 2), lax.rem(j + 2, 4)


def at(start, size):
    return pl.ds(pl.multiple_of(start, 128), size)


def call(body, outs, args, flops, in_place=(), scratch=(), vmem=VMEM_SMALL):
    bytes_moved = sum(a.size * a.dtype.itemsize for a in args) + sum(
        np.prod(s) * np.dtype(d).itemsize for s, d in outs
    )
    return pl.pallas_call(
        body,
        out_shape=[jax.ShapeDtypeStruct(s, d) for s, d in outs],
        in_specs=[
            pl.BlockSpec(memory_space=pltpu.HBM if i in in_place else pltpu.VMEM)
            for i in range(len(args))
        ],
        out_specs=[pl.BlockSpec(memory_space=pltpu.VMEM)] * len(outs),
        scratch_shapes=list(scratch),
        cost_estimate=pl.CostEstimate(
            flops=int(flops), bytes_accessed=int(bytes_moved), transcendentals=0
        ),
        compiler_params=pltpu.CompilerParams(vmem_limit_bytes=vmem),
    )(*args)


def slot_parts(i):
    who = lax.shift_right_logical(i * 2731, 16)
    rest = i - who * 24
    part = lax.shift_right_logical(rest * 43, 8)
    return who, part, rest - part * 6


def half_copy(from_ref, to_ref, sem, half):
    return pltpu.make_async_copy(from_ref.at[:, at(half * HALF, HALF)], to_ref, sem)


def pick_rows(code_first, code_second, row_class, data, send_ref, weights=None):
    step = 384
    who, part, rank = slot_parts(lax.broadcasted_iota(jnp.int32, (step, TOK), 0))
    base = who * CAP + rank
    for k in range(SLOTS // step):
        target = base + (k * (step // 24) * CAP + row_class * SUB)
        hit_first = target == code_first
        hit_second = target == code_second
        pick = jnp.where(hit_first, 1.0, jnp.where(hit_second, 1.0, 0.0))
        picks = jnp.concatenate(
            [jnp.where(part == q, pick, 0.0).astype(BF) for q in range(4)], axis=1
        )
        rows = dot(picks, data)
        if weights is not None:
            rows = rows * jnp.sum(
                jnp.where(hit_first, weights[0:1, :], 0.0)
                + jnp.where(hit_second, weights[1:2, :], 0.0),
                axis=1,
                keepdims=True,
            )
        send_ref[k * step : (k + 1) * step, :] = rows.astype(BF)


def stacked_quarters(buffer):
    return jnp.concatenate([buffer[:, q * 256 : (q + 1) * 256] for q in range(4)], axis=0)


def pack_input_body(routes_ref, input_ref, send_ref, row_ref, buffer, sem):
    _, half, row_class = spot()
    copy = half_copy(input_ref, buffer, sem, half)
    copy.start()
    experts = lax.broadcasted_iota(jnp.int32, (EXPERTS, TOK), 0)
    first, second = routes_ref[0:1, :], routes_ref[1:2, :]
    before = lax.broadcasted_iota(jnp.int32, (TOK, TOK), 0) < lax.broadcasted_iota(
        jnp.int32, (TOK, TOK), 1
    )
    before = jnp.where(before, 1.0, 0.0).astype(BF)
    one_first = jnp.where(experts == first, 1.0, 0.0)
    one_second = jnp.where(experts == second, 1.0, 0.0)
    count_first = dot(one_first.astype(BF), before)
    count_second = dot(one_second.astype(BF), before) + jnp.sum(one_first, axis=1, keepdims=True)
    rank_first = jnp.sum(one_first * count_first, axis=0, keepdims=True).astype(jnp.int32)
    rank_second = jnp.sum(one_second * count_second, axis=0, keepdims=True).astype(jnp.int32)
    code_first = first * CAP + rank_first
    code_second = second * CAP + rank_second
    row_ref[0:1, :] = code_first
    row_ref[1:2, :] = code_second
    copy.wait()
    pick_rows(code_first, code_second, row_class, stacked_quarters(buffer[...]), send_ref)


def pack_grad_body(row_ref, weight_ref, grad_ref, send_ref, code_ref, cols_ref, buffer, sem):
    j, half, row_class = spot()
    copy = half_copy(grad_ref, buffer, sem, half)
    copy.start()
    code_first, code_second = row_ref[0:1, :], row_ref[1:2, :]
    codes = jnp.concatenate(
        [
            jnp.broadcast_to(code_first.astype(F32), (64, TOK)),
            jnp.broadcast_to(code_second.astype(F32), (64, TOK)),
        ],
        axis=0,
    )
    code_ref[...] = jnp.transpose(codes)
    copy.wait()
    cols_ref[...] = buffer[:, at(lax.rem(j, 2) * QUART, QUART)]
    pick_rows(
        code_first,
        code_second,
        row_class,
        stacked_quarters(buffer[...]),
        send_ref,
        weight_ref[...],
    )


def unpack_body(recv_ref, perm_ref, *out_refs):
    each = 8 // len(out_refs)
    for group in range(8):
        rows = dot(perm_ref[...], recv_ref[group * 192 : (group + 1) * 192, :]).astype(BF)
        out_ref = out_refs[group // each]
        to = slice(group % each * 48, (group % each + 1) * 48)
        for q in range(4):
            out_ref[to, q * 256 : (q + 1) * 256] = rows[q * 48 : (q + 1) * 48]


def whole_rows(own_ref, other_ref, half, out_ref):
    out_ref[:, at(half * HALF, HALF)] = own_ref[...]
    out_ref[:, at((1 - half) * HALF, HALF)] = other_ref[...]


def forward_body(own_ref, other_ref, wg_ref, wg2_ref, wu_ref, wu2_ref, x_ref, *out_refs):
    _, half, _ = spot()
    whole_rows(own_ref, other_ref, half, x_ref)
    x = x_ref[...]
    for k, w_ref in enumerate((wg_ref, wg2_ref, wu_ref, wu2_ref)):
        made = dot(x, w_ref[...])
        cols = slice(k % 2 * HID, (k % 2 + 1) * HID)
        out_refs[k // 2][:, cols] = made[0:PART]
        out_refs[2 + k // 2][:, cols] = made[PART:ROWS]


def partial_rows(gd, ud, gd2, ud2, wg_ref, wg2_ref, wu_ref, wu2_ref, start):
    rows = at(start, HALF)
    return (
        dotg(gd, wg_ref[rows, :], NT)
        + dotg(ud, wu_ref[rows, :], NT)
        + dotg(gd2, wg2_ref[rows, :], NT)
        + dotg(ud2, wu2_ref[rows, :], NT)
    )


def delta_body(
    own_ref, other_ref, gate_ref, up_ref, wd_ref, wd2_ref, wg_ref, wg2_ref, wu_ref, wu2_ref,
    g_ref, h_ref, h2_ref, gd_ref, gd2_ref, ud_ref, ud2_ref, send_ref, down_buf, in_buf, sems,
):
    _, half, _ = spot()
    start = pl.multiple_of((1 - half) * HALF, HALF)
    copies = [
        pltpu.make_async_copy(ref, down_buf.at[k], sems.at[k])
        for k, ref in enumerate((wd_ref, wd2_ref))
    ] + [
        pltpu.make_async_copy(ref.at[pl.ds(start, HALF), :], in_buf.at[k], sems.at[2 + k])
        for k, ref in enumerate((wg_ref, wu_ref, wg2_ref, wu2_ref))
    ]
    for copy in copies:
        copy.start()
    whole_rows(own_ref, other_ref, half, g_ref)
    g = g_ref[...]
    total = jnp.zeros((PART, HALF), F32)
    for k, (ho, go, uo) in enumerate(((h_ref, gd_ref, ud_ref), (h2_ref, gd2_ref, ud2_ref))):
        copies[k].wait()
        act_grad = dotg(g, down_buf[k], NT)
        gate = gate_ref[:, k * HID : (k + 1) * HID]
        up = up_ref[:, k * HID : (k + 1) * HID]
        sigma = jax.nn.sigmoid(gate)
        act = gate * sigma
        ho[...] = (act * up).astype(BF)
        go[...] = (act_grad * up * (sigma * (1.0 + gate * (1.0 - sigma)))).astype(BF)
        uo[...] = (act_grad * act).astype(BF)
    for k, ref in enumerate((gd_ref, ud_ref, gd2_ref, ud2_ref)):
        copies[2 + k].wait()
        total = total + dotg(ref[...], in_buf[k], NT)
    send_ref[...] = total.astype(BF)


def join_body(*refs):
    count = len(refs) // 3
    for k in range(count):
        refs[2 * count + k][0:PART, :] = refs[k][...]
        refs[2 * count + k][PART:ROWS, :] = refs[count + k][...]


def keep_body(gd_ref, gd2_ref, ud_ref, ud2_ref, wg_ref, wg2_ref, wu_ref, wu2_ref, keep_ref):
    _, half, _ = spot()
    keep_ref[...] = partial_rows(
        gd_ref[...], ud_ref[...], gd2_ref[...], ud2_ref[...],
        wg_ref, wg2_ref, wu_ref, wu2_ref, half * HALF,
    )


def back_body(keep_ref, first_ref, second_ref, perm_ref, send_ref):
    for group in range(8):
        rows = slice(group * 48, (group + 1) * 48)
        recv_ref = second_ref if group >= 4 else first_ref
        recv = recv_ref[group % 4 * 48 : (group % 4 + 1) * 48, :]
        total = (keep_ref[rows, :] + recv.astype(F32)).astype(BF)
        stacked = jnp.concatenate([total[:, q * 256 : (q + 1) * 256] for q in range(4)], axis=0)
        send_ref[group * 192 : (group + 1) * 192, :] = dot(perm_ref[...], stacked).astype(BF)


def combine_body(back_ref, code_ref, grad_ref, keep_ref, send_ref):
    j, _, row_class = spot()
    who, part, rank = slot_parts(lax.broadcasted_iota(jnp.int32, (1, SLOTS), 1))
    target = (who * CAP + rank + row_class * SUB).astype(F32)
    hit = jnp.where(
        target == code_ref[:, 0:1], 1.0, jnp.where(target == code_ref[:, 64:65], 1.0, 0.0)
    )
    kept = lax.rem(j, 2) * 2
    back = back_ref[...]
    for a in range(2):
        theirs = dot(jnp.where(part == 2 - kept + a, hit, 0.0).astype(BF), back)
        send_ref[:, a * 256 : (a + 1) * 256] = theirs.astype(BF)
    for a in range(2):
        cols = slice(a * 256, (a + 1) * 256)
        mine = dot(jnp.where(part == kept + a, hit, 0.0).astype(BF), back)
        keep_ref[:, cols] = grad_ref[:, cols].astype(F32) + mine


def aux_body(proj_ref, hat_ref, gain_ref, *out_refs):
    j, _, _ = spot()
    gain = gain_ref[...]
    top = gain.astype(BF)
    rest = gain - top.astype(F32)
    mid = rest.astype(BF)
    low = (rest - mid.astype(F32)).astype(BF)
    row = lax.broadcasted_iota(jnp.int32, (16, CH), 0)
    gains = jnp.where(
        row == 0,
        top.astype(F32),
        jnp.where(row == 1, mid.astype(F32), jnp.where(row == 2, low.astype(F32), 0.0)),
    ).astype(BF)
    for to, out_ref in zip((j, *peers(j)), out_refs):
        out_ref[0:512, :] = proj_ref[pl.ds(pl.multiple_of(to * 512, 512), 512), :]
        out_ref[512:768, :] = hat_ref[...]
        out_ref[768:784, :] = gains


def channel_body(
    own_ref, across_ref, beside_ref, opposite_ref, row_ref, proj_ref, act_ref, slope_ref, hat_ref, rstd_ref
):
    rstd_ref[...] = jnp.transpose(jnp.broadcast_to(row_ref[...], (128, TOK)))
    j, _, _ = spot()
    for owner, ref in zip((j, *peers(j)), (own_ref, across_ref, beside_ref, opposite_ref)):
        cols = at(owner * CH, CH)
        proj_ref[:, cols] = ref[0:512, :]
        hat = ref[512:768, :]
        gains = ref[768:784, :].astype(F32)
        gain = gains[0:1, :] + gains[1:2, :] + gains[2:3, :]
        normed = hat.astype(F32) * gain
        sigma = jax.nn.sigmoid(normed)
        hat_ref[:, cols] = hat
        act_ref[:, cols] = (normed * sigma).astype(BF)
        slope_ref[:, cols] = sigma * (1.0 + normed * (1.0 - sigma)) * gain


def mixed(keep_ref, recv_ref):
    return (keep_ref[...] + recv_ref[...].astype(F32)).astype(BF)


def outer_body(keep_ref, recv_ref, act_ref, own_ref, other_ref, turned_ref):
    mix = mixed(keep_ref, recv_ref)
    turned_ref[...] = jnp.transpose(mix.astype(F32))
    core = lax.rem(lax.axis_index("sp"), 2)

    def rows_of(parity):
        return jnp.concatenate(
            [
                turned_ref[pl.ds(pl.multiple_of((2 * b + parity) * 32, 32), 32), :]
                for b in range(8)
            ],
            axis=0,
        ).astype(BF)

    theirs, mine = rows_of(1 - core), rows_of(core)
    for k in range(4):
        act = act_ref[:, k * CH : (k + 1) * CH]
        other_ref[k * 256 : (k + 1) * 256, :] = dot(theirs, act).astype(BF)
        own_ref[k * 256 : (k + 1) * 256, :] = dot(mine, act)


def sum_body(own_ref, recv_ref, out_ref):
    out_ref[...] = (own_ref[...] + recv_ref[...].astype(F32)).astype(BF)


def silu_body(keep_ref, recv_ref, proj_ref, slope_ref, hat_ref, *refs):
    j, _, _ = spot()
    out_refs, part_ref = refs[:4], refs[4]
    mix = mixed(keep_ref, recv_ref)
    part = dot(mix, proj_ref[...])
    sloped = part * slope_ref[...]
    dotted = sloped * hat_ref[...].astype(F32)
    ones = jnp.ones((16, 4 * CH), BF)
    total = dotg(ones, sloped.astype(BF), NT)
    total_dot = dotg(ones, dotted.astype(BF), NT)
    row = lax.broadcasted_iota(jnp.int32, (16, TOK), 0)
    top, top_dot = total.astype(BF).astype(F32), total_dot.astype(BF).astype(F32)
    sums = jnp.where(
        row == 0,
        top,
        jnp.where(
            row == 1,
            total - top,
            jnp.where(row == 2, top_dot, jnp.where(row == 3, total_dot - top_dot, 0.0)),
        ),
    ).astype(BF)
    part_ref[...] = part
    for d, out_ref in enumerate(out_refs):
        out_ref[0:256, :] = part_ref[:, at(lax.rem(j + d, 4) * CH, CH)].astype(BF)
        out_ref[256:272, :] = sums


def conv_body(r0_ref, r1_ref, r2_ref, r3_ref, slope_ref, hat_ref, rstd_ref, out_ref, head_ref):
    j, _, _ = spot()
    recv_refs = (r0_ref, r1_ref, r2_ref, r3_ref)
    total = sum(ref[0:256, :].astype(F32) for ref in recv_refs)
    rows = jnp.concatenate([ref[256:272, :] for ref in recv_refs], axis=0)
    kind = lax.rem(lax.broadcasted_iota(jnp.int32, (64, CH), 0), 16)
    pick = jnp.where(kind < 2, 1.0, 0.0).astype(BF)
    pick_dot = jnp.where(kind < 2, 0.0, jnp.where(kind < 4, 1.0, 0.0)).astype(BF)
    mean = dotg(rows, pick, TN) * (1.0 / (4 * CH))
    mean_dot = dotg(rows, pick_dot, TN) * (1.0 / (4 * CH))
    hat_grad = total * slope_ref[:, at(j * CH, CH)]
    out_ref[...] = rstd_ref[:, 0:1] * (hat_grad - mean - hat_ref[...].astype(F32) * mean_dot)
    head_ref[...] = out_ref[0:32, :]


def taps_body(grad_ref, next_ref, taps_ref, gate_ref, value_ref, out_ref, gate_out_ref, long_ref):
    long_ref[0:256, :] = grad_ref[...]
    long_ref[256:288, :] = next_ref[...]
    for block in range(4):
        row = block * 64
        total = jnp.zeros((64, CH), F32)
        for k in range(31):
            tap = taps_ref[k : k + 1, :].astype(F32)
            total = total + tap * long_ref[row + 30 - k : row + 94 - k, :]
        rows = slice(row, row + 64)
        sigma = jax.nn.sigmoid(gate_ref[rows, :].astype(F32))
        out_ref[rows, :] = (total * sigma).astype(BF)
        gate_out_ref[rows, :] = (
            total * value_ref[rows, :].astype(F32) * sigma * (1.0 - sigma)
        ).astype(BF)


def around(blocks):
    return [lax.ppermute(blocks[d], "tp", [(i, (i + d) % 4) for i in range(4)]) for d in (1, 3, 2)]


def exchanged(array, **groups):
    return lax.all_to_all(array, "sp", split_axis=0, concat_axis=0, tiled=True, **groups)


def unmix_matrix():
    m = np.zeros((192, 192), np.float32)
    for q in range(4):
        for s in range(8):
            for r in range(6):
                m[q * 48 + s * 6 + r, s * 24 + q * 6 + r] = 1.0
    return m


def on_device(
    moe_input,
    out_cotangent,
    routes,
    group_weight,
    inner_weight,
    gate_weight,
    up_weight,
    down_weight,
    value_in,
    gate_in,
    conv_taps,
    norm_hat,
    norm_rstd,
    norm_gain,
    out_proj,
):
    sp_count = lax.axis_size("sp")
    unmix = unmix_matrix()
    unmix_to = jnp.asarray(unmix, BF)
    unmix_from = jnp.asarray(unmix.T, BF)
    wg, wu, wd = gate_weight[0], up_weight[0], down_weight[0]
    wg2 = lax.ppermute(wg, "tp", PAIR_W)
    wu2 = lax.ppermute(wu, "tp", PAIR_W)
    wd2 = lax.ppermute(wd, "tp", PAIR_W)

    route_weight = group_weight[None, :] * inner_weight.T
    buffer = [pltpu.VMEM((TOK, HALF), BF), pltpu.SemaphoreType.DMA]
    x_send, code_rows = call(
        pack_input_body,
        [((SLOTS, 256), BF), ((2, TOK), jnp.int32)],
        (routes.T, moe_input),
        2 * SLOTS * 1024 * 256,
        vmem=VMEM_WHOLE,
        in_place=(1,),
        scratch=buffer,
    )
    g_send, codes, own_cols = call(
        pack_grad_body,
        [((SLOTS, 256), BF), ((TOK, 128), F32), ((TOK, QUART), BF)],
        (code_rows, route_weight, out_cotangent),
        2 * SLOTS * 1024 * 256,
        in_place=(2,),
        scratch=buffer,
    )

    blocks = call(
        aux_body,
        [((AUX, CH), BF)] * 4,
        (out_proj, norm_hat, norm_gain[None, :]),
        0,
    )
    across = lax.ppermute(blocks[1], "tp", PAIR_R)
    relayed = lax.ppermute(blocks[3], "tp", PAIR_R)
    beside = lax.ppermute(blocks[2], "tp", PAIR_W)
    opposite = lax.ppermute(relayed, "tp", PAIR_W)
    proj_rows, act, slope, hat, rstd = call(
        channel_body,
        [((512, 4 * CH), BF), ((TOK, 4 * CH), BF), ((TOK, 4 * CH), F32), ((TOK, 4 * CH), BF), ((TOK, 128), F32)],
        (blocks[0], across, beside, opposite, norm_rstd[None, :]),
        0,
    )

    def dispatched(send, parts):
        recv = exchanged(send.reshape(sp_count, 24, 256))
        own = call(
            unpack_body,
            [((ROWS // parts, HALF), BF)] * parts,
            (recv.reshape(SLOTS, 256), unmix_to),
            2 * SLOTS * 192 * 256,
        )
        return own, [lax.ppermute(v, "tp", PAIR_R) for v in own]

    (x_own,), (x_other,) = dispatched(x_send, 1)
    g_own, g_other = dispatched(g_send, 2)
    x, *pre = call(
        forward_body,
        [((ROWS, WIDTH), BF)] + [((PART, 2 * HID), F32)] * 4,
        (x_own, x_other, wg, wg2, wu, wu2),
        2 * ROWS * WIDTH * 4 * HID,
        vmem=VMEM_LARGE,
    )
    halves, rows_recv = [], []
    for k in range(2):
        *made, rows_send = call(
            delta_body,
            [((PART, WIDTH), BF)] + [((PART, HID), BF)] * 6 + [((PART, HALF), BF)],
            (g_own[k], g_other[k], pre[2 * k], pre[2 * k + 1], wd, wd2, wg, wg2, wu, wu2),
            2 * PART * WIDTH * 4 * HID,
            in_place=range(4, 10),
            scratch=[pltpu.VMEM((2, HID, WIDTH), BF), pltpu.VMEM((4, HALF, HID), BF)]
            + [pltpu.SemaphoreType.DMA((6,))],
            vmem=VMEM_LARGE,
        )
        halves += made
        rows_recv.append(lax.ppermute(rows_send, "tp", PAIR_R))
    g, h, h2, gd, gd2, ud, ud2 = call(
        join_body,
        [((ROWS, WIDTH), BF)] + [((ROWS, HID), BF)] * 6,
        halves,
        0,
    )
    (rows_keep,) = call(
        keep_body,
        [((ROWS, HALF), F32)],
        (gd, gd2, ud, ud2, wg, wg2, wu, wu2),
        2 * ROWS * HALF * 4 * HID,
        vmem=VMEM_LARGE,
    )

    def outer(a, b):
        return lax.dot_general(a, b, TN, preferred_element_type=F32)

    def finished(a, b, b_other):
        other = outer(*b_other).astype(BF)
        arrived = lax.ppermute(other, "tp", PAIR_W)
        return (outer(a, b) + arrived.astype(F32)).astype(BF)[None]

    gate_grad = finished(x, gd, (x, gd2))
    up_grad = finished(x, ud, (x, ud2))
    down_own = lax.optimization_barrier(outer(h, g))
    down_arrived = []
    for k in range(2):
        part = outer(h2[:, k * 128 : (k + 1) * 128], g).astype(BF)
        down_arrived.append(lax.ppermute(part, "tp", PAIR_W))
    down_grad = (down_own + jnp.concatenate(down_arrived).astype(F32)).astype(BF)[None]

    (back_send,) = call(
        back_body,
        [((SLOTS, 256), BF)],
        (rows_keep, *rows_recv, unmix_from),
        2 * SLOTS * 192 * 256,
    )
    back = exchanged(back_send.reshape(sp_count, 24, 256))

    mix_keep, mix_send = call(
        combine_body,
        [((TOK, QUART), F32), ((TOK, QUART), BF)],
        (back.reshape(SLOTS, 256), codes, own_cols),
        2 * SLOTS * 1024 * 256,
    )
    mix_recv = lax.ppermute(mix_send, "tp", PAIR_W)
    outer_own, outer_other = call(
        outer_body,
        [((1024, CH), F32), ((1024, CH), BF)],
        (mix_keep, mix_recv, act),
        2 * TOK * 512 * 1024,
        scratch=[pltpu.VMEM((512, TOK), F32)],
    )
    outer_recv = lax.ppermute(outer_other, "sp", [(i, i ^ 1) for i in range(sp_count)])
    (outer_sum,) = call(sum_body, [((1024, CH), BF)], (outer_own, outer_recv), 0)
    pieces = exchanged(
        outer_sum.reshape(sp_count // 2, 32, CH),
        axis_index_groups=[list(range(c, sp_count, 2)) for c in range(2)],
    )
    piece = jnp.sum(pieces.astype(F32), axis=0)
    per_tp = sp_count // 4
    proj_grad = lax.ppermute(
        piece,
        ("sp", "tp"),
        [
            (s * 4 + t, (per_tp * t + s % per_tp) * 4 + s // per_tp)
            for s in range(sp_count)
            for t in range(4)
        ],
    )

    silu_parts = call(
        silu_body,
        [((272, CH), BF)] * 4,
        (mix_keep, mix_recv, proj_rows, slope, hat),
        2 * TOK * 512 * 1024,
        scratch=[pltpu.VMEM((TOK, 4 * CH), F32)],
    )
    silu_parts = [silu_parts[0]] + around(silu_parts)
    conv_grad, head = call(
        conv_body,
        [((TOK, CH), F32), ((32, CH), F32)],
        (*silu_parts, slope, norm_hat, rstd),
        0,
    )
    incoming = lax.ppermute(head, "sp", [(i, i - 1) for i in range(1, sp_count)])
    value_grad, gate_in_grad = call(
        taps_body,
        [((TOK, CH), BF), ((TOK, CH), BF)],
        (conv_grad, incoming, conv_taps, gate_in, value_in),
        0,
        scratch=[pltpu.VMEM((TOK + 32, CH), F32)],
    )
    return (gate_grad, up_grad, down_grad, proj_grad, value_grad, gate_in_grad)


def solution(mesh):
    return jax.shard_map(
        on_device,
        mesh=mesh,
        in_specs=(
            P("sp", None),
            P("sp", None),
            P("sp", None),
            P("sp"),
            P("sp", None),
            P("sp", None, "tp"),
            P("sp", None, "tp"),
            P("sp", "tp", None),
            P("sp", "tp"),
            P("sp", "tp"),
            P(None, "tp"),
            P("sp", "tp"),
            P("sp"),
            P("tp"),
            P(None, "tp"),
        ),
        out_specs=(
            P("sp", None, "tp"),
            P("sp", None, "tp"),
            P("sp", "tp", None),
            P("sp", "tp"),
            P("sp", "tp"),
            P("sp", "tp"),
        ),
        check_vma=False,
    )
```

```python
import jax
import jax.numpy as jnp
import numpy as np
from jax import lax
from jax.experimental import pallas as pl
from jax.experimental.pallas import tpu as pltpu
from jax.sharding import PartitionSpec as P


BF = jnp.bfloat16
F32 = jnp.float32
TOK = 256
WIDTH = 2048
HALF = 1024
QUART = 512
CH = 256
HID = 256
EXPERTS = 64
CAP = 12
SUB = 6
ROWS = 64 * SUB
PART = ROWS // 2
SLOTS = 64 * 24
AUX = 512 + 256 + 16
VMEM_SMALL = 16 * 1024 * 1024
VMEM_LARGE = 24 * 1024 * 1024
VMEM_WHOLE = 60 * 1024 * 1024
SP, TP = "sp", "tp"
PAIR_W = [(0, 1), (1, 0), (2, 3), (3, 2)]
PAIR_R = [(0, 3), (3, 0), (1, 2), (2, 1)]

NT = (((1,), (1,)), ((), ()))
TN = (((0,), (0,)), ((), ()))


def dot(a, b):
    return jnp.dot(a, b, preferred_element_type=F32)


def dotg(a, b, dims):
    return lax.dot_general(a, b, dims, preferred_element_type=F32)


def spot():
    j = lax.axis_index(TP)
    half = lax.shift_right_logical(j, 1)
    row_class = lax.rem(lax.shift_right_logical(j + 1, 1), 2)
    return j, half, row_class


def peers(j):
    return 3 - j, j + 1 - 2 * lax.rem(j, 2), lax.rem(j + 2, 4)


def at(start, size):
    return pl.ds(pl.multiple_of(start, 128), size)


def call(body, outs, args, flops, in_place=(), scratch=(), vmem=VMEM_SMALL):
    bytes_moved = sum(a.size * a.dtype.itemsize for a in args) + sum(
        np.prod(s) * np.dtype(d).itemsize for s, d in outs
    )
    return pl.pallas_call(
        body,
        out_shape=[jax.ShapeDtypeStruct(s, d) for s, d in outs],
        in_specs=[
            pl.BlockSpec(memory_space=pltpu.HBM if i in in_place else pltpu.VMEM)
            for i in range(len(args))
        ],
        out_specs=[pl.BlockSpec(memory_space=pltpu.VMEM)] * len(outs),
        scratch_shapes=list(scratch),
        cost_estimate=pl.CostEstimate(
            flops=int(flops), bytes_accessed=int(bytes_moved), transcendentals=0
        ),
        compiler_params=pltpu.CompilerParams(vmem_limit_bytes=vmem),
    )(*args)


def slot_parts(i):
    who = lax.shift_right_logical(i * 2731, 16)
    rest = i - who * 24
    part = lax.shift_right_logical(rest * 43, 8)
    return who, part, rest - part * 6


def half_copy(from_ref, to_ref, sem, half):
    return pltpu.make_async_copy(from_ref.at[:, at(half * HALF, HALF)], to_ref, sem)


def pick_rows(code_first, code_second, row_class, data, send_ref, weights=None):
    step = 384
    who, part, rank = slot_parts(lax.broadcasted_iota(jnp.int32, (step, TOK), 0))
    base = who * CAP + rank
    for k in range(SLOTS // step):
        target = base + (k * (step // 24) * CAP + row_class * SUB)
        hit_first = target == code_first
        hit_second = target == code_second
        pick = jnp.where(hit_first, 1.0, jnp.where(hit_second, 1.0, 0.0))
        picks = jnp.concatenate(
            [jnp.where(part == q, pick, 0.0).astype(BF) for q in range(4)], axis=1
        )
        rows = dot(picks, data)
        if weights is not None:
            rows = rows * jnp.sum(
                jnp.where(hit_first, weights[0:1, :], 0.0)
                + jnp.where(hit_second, weights[1:2, :], 0.0),
                axis=1,
                keepdims=True,
            )
        send_ref[k * step : (k + 1) * step, :] = rows.astype(BF)


def stacked_quarters(buffer):
    return jnp.concatenate([buffer[:, q * 256 : (q + 1) * 256] for q in range(4)], axis=0)


def pack_x_body(routes_ref, input_ref, send_ref, row_ref, buffer, sem):
    _, half, row_class = spot()
    copy = half_copy(input_ref, buffer, sem, half)
    copy.start()
    experts = lax.broadcasted_iota(jnp.int32, (EXPERTS, TOK), 0)
    first, second = routes_ref[0:1, :], routes_ref[1:2, :]
    before = lax.broadcasted_iota(jnp.int32, (TOK, TOK), 0) < lax.broadcasted_iota(
        jnp.int32, (TOK, TOK), 1
    )
    before = jnp.where(before, 1.0, 0.0).astype(BF)
    one_first = jnp.where(experts == first, 1.0, 0.0)
    one_second = jnp.where(experts == second, 1.0, 0.0)
    count_first = dot(one_first.astype(BF), before)
    count_second = dot(one_second.astype(BF), before) + jnp.sum(one_first, axis=1, keepdims=True)
    rank_first = jnp.sum(one_first * count_first, axis=0, keepdims=True).astype(jnp.int32)
    rank_second = jnp.sum(one_second * count_second, axis=0, keepdims=True).astype(jnp.int32)
    code_first = first * CAP + rank_first
    code_second = second * CAP + rank_second
    row_ref[0:1, :] = code_first
    row_ref[1:2, :] = code_second
    copy.wait()
    pick_rows(code_first, code_second, row_class, stacked_quarters(buffer[...]), send_ref)


def pack_g_body(row_ref, weight_ref, grad_ref, send_ref, cols_ref, buffer, sem):
    j, half, row_class = spot()
    copy = half_copy(grad_ref, buffer, sem, half)
    copy.start()
    code_first, code_second = row_ref[0:1, :], row_ref[1:2, :]
    codes = jnp.concatenate(
        [
            jnp.broadcast_to(code_first.astype(F32), (64, TOK)),
            jnp.broadcast_to(code_second.astype(F32), (64, TOK)),
        ],
        axis=0,
    )
    codes = jnp.transpose(codes)
    high = jnp.floor(codes * (1.0 / 256.0))
    lane = lax.broadcasted_iota(jnp.int32, (TOK, 128), 1)
    split = jnp.where(lax.rem(lane, 2) == 0, codes - 256.0 * high, high)
    cols_ref[:, QUART : QUART + 128] = split.astype(BF)
    copy.wait()
    cols_ref[:, 0:QUART] = buffer[:, at(lax.rem(j, 2) * QUART, QUART)]
    pick_rows(
        code_first,
        code_second,
        row_class,
        stacked_quarters(buffer[...]),
        send_ref,
        weight_ref[...],
    )


def unpack_body(recv_ref, perm_ref, *out_refs):
    each = 8 // len(out_refs)
    for group in range(8):
        rows = dot(perm_ref[...], recv_ref[group * 192 : (group + 1) * 192, :]).astype(BF)
        out_ref = out_refs[group // each]
        to = slice(group % each * 48, (group % each + 1) * 48)
        for q in range(4):
            out_ref[to, q * 256 : (q + 1) * 256] = rows[q * 48 : (q + 1) * 48]


def whole_rows(own_ref, other_ref, half, out_ref):
    out_ref[:, at(half * HALF, HALF)] = own_ref[...]
    out_ref[:, at((1 - half) * HALF, HALF)] = other_ref[...]


def forward_body(own_ref, other_ref, wg_ref, wg2_ref, wu_ref, wu2_ref, x_ref, *out_refs):
    _, half, _ = spot()
    whole_rows(own_ref, other_ref, half, x_ref)
    x = x_ref[...]
    for k, w_ref in enumerate((wg_ref, wg2_ref, wu_ref, wu2_ref)):
        made = dot(x, w_ref[...])
        cols = slice(k % 2 * HID, (k % 2 + 1) * HID)
        out_refs[k // 2][:, cols] = made[0:PART]
        out_refs[2 + k // 2][:, cols] = made[PART:ROWS]


def partial_rows(gd, ud, gd2, ud2, wg_ref, wg2_ref, wu_ref, wu2_ref, start):
    rows = at(start, HALF)
    return (
        dotg(gd, wg_ref[rows, :], NT)
        + dotg(ud, wu_ref[rows, :], NT)
        + dotg(gd2, wg2_ref[rows, :], NT)
        + dotg(ud2, wu2_ref[rows, :], NT)
    )


def delta_body(
    own_ref, other_ref, gate_ref, up_ref, wd_ref, wd2_ref, wg_ref, wg2_ref, wu_ref, wu2_ref,
    g_ref, h_ref, h2_ref, gd_ref, gd2_ref, ud_ref, ud2_ref, send_ref, down_buf, in_buf, sems,
):
    _, half, _ = spot()
    start = pl.multiple_of((1 - half) * HALF, HALF)
    copies = [
        pltpu.make_async_copy(ref, down_buf.at[k], sems.at[k])
        for k, ref in enumerate((wd_ref, wd2_ref))
    ] + [
        pltpu.make_async_copy(ref.at[pl.ds(start, HALF), :], in_buf.at[k], sems.at[2 + k])
        for k, ref in enumerate((wg_ref, wu_ref, wg2_ref, wu2_ref))
    ]
    for copy in copies:
        copy.start()
    whole_rows(own_ref, other_ref, half, g_ref)
    g = g_ref[...]
    total = jnp.zeros((PART, HALF), F32)
    for k, (ho, go, uo) in enumerate(((h_ref, gd_ref, ud_ref), (h2_ref, gd2_ref, ud2_ref))):
        copies[k].wait()
        act_grad = dotg(g, down_buf[k], NT)
        gate = gate_ref[:, k * HID : (k + 1) * HID]
        up = up_ref[:, k * HID : (k + 1) * HID]
        sigma = jax.nn.sigmoid(gate)
        act = gate * sigma
        ho[...] = (act * up).astype(BF)
        go[...] = (act_grad * up * (sigma * (1.0 + gate * (1.0 - sigma)))).astype(BF)
        uo[...] = (act_grad * act).astype(BF)
    for k, ref in enumerate((gd_ref, ud_ref, gd2_ref, ud2_ref)):
        copies[2 + k].wait()
        total = total + dotg(ref[...], in_buf[k], NT)
    send_ref[...] = total.astype(BF)


def join_body(*refs):
    count = len(refs) // 3
    for k in range(count):
        refs[2 * count + k][0:PART, :] = refs[k][...]
        refs[2 * count + k][PART:ROWS, :] = refs[count + k][...]


def keep_body(gd_ref, gd2_ref, ud_ref, ud2_ref, wg_ref, wg2_ref, wu_ref, wu2_ref, keep_ref):
    _, half, _ = spot()
    keep_ref[...] = partial_rows(
        gd_ref[...], ud_ref[...], gd2_ref[...], ud2_ref[...],
        wg_ref, wg2_ref, wu_ref, wu2_ref, half * HALF,
    )


def back_pack_body(keep_ref, first_ref, second_ref, perm_ref, send_ref):
    for group in range(8):
        rows = slice(group * 48, (group + 1) * 48)
        recv_ref = second_ref if group >= 4 else first_ref
        recv = recv_ref[group % 4 * 48 : (group % 4 + 1) * 48, :]
        total = (keep_ref[rows, :] + recv.astype(F32)).astype(BF)
        stacked = jnp.concatenate([total[:, q * 256 : (q + 1) * 256] for q in range(4)], axis=0)
        send_ref[group * 192 : (group + 1) * 192, :] = dot(perm_ref[...], stacked).astype(BF)


def combine_body(back_ref, cols_ref, keep_ref, send_ref):
    j, _, row_class = spot()
    who, part, rank = slot_parts(lax.broadcasted_iota(jnp.int32, (1, SLOTS), 1))
    target = (who * CAP + rank + row_class * SUB).astype(F32)
    codes = cols_ref[:, QUART : QUART + 128].astype(F32)
    code_first = codes[:, 0:1] + 256.0 * codes[:, 1:2]
    code_second = codes[:, 64:65] + 256.0 * codes[:, 65:66]
    hit = jnp.where(target == code_first, 1.0, jnp.where(target == code_second, 1.0, 0.0))
    kept = lax.rem(j, 2) * 2
    back = back_ref[...]
    for a in range(2):
        theirs = dot(jnp.where(part == 2 - kept + a, hit, 0.0).astype(BF), back)
        send_ref[:, a * 256 : (a + 1) * 256] = theirs.astype(BF)
    for a in range(2):
        cols = slice(a * 256, (a + 1) * 256)
        mine = dot(jnp.where(part == kept + a, hit, 0.0).astype(BF), back)
        keep_ref[:, cols] = cols_ref[:, cols].astype(F32) + mine


def aux_body(proj_ref, hat_ref, gain_ref, *out_refs):
    j, _, _ = spot()
    gain = gain_ref[...]
    top = gain.astype(BF)
    rest = gain - top.astype(F32)
    mid = rest.astype(BF)
    low = (rest - mid.astype(F32)).astype(BF)
    row = lax.broadcasted_iota(jnp.int32, (16, CH), 0)
    gains = jnp.where(
        row == 0,
        top.astype(F32),
        jnp.where(row == 1, mid.astype(F32), jnp.where(row == 2, low.astype(F32), 0.0)),
    ).astype(BF)
    for to, out_ref in zip((j, *peers(j)), out_refs):
        out_ref[0:512, :] = proj_ref[pl.ds(pl.multiple_of(to * 512, 512), 512), :]
        out_ref[512:768, :] = hat_ref[...]
        out_ref[768:784, :] = gains


def channel_body(
    own_ref, across_ref, beside_ref, opposite_ref, row_ref, proj_ref, act_ref, slope_ref, hat_ref, rstd_ref
):
    rstd_ref[...] = jnp.transpose(jnp.broadcast_to(row_ref[...], (128, TOK)))
    j, _, _ = spot()
    for owner, ref in zip((j, *peers(j)), (own_ref, across_ref, beside_ref, opposite_ref)):
        cols = at(owner * CH, CH)
        proj_ref[:, cols] = ref[0:512, :]
        hat = ref[512:768, :]
        gains = ref[768:784, :].astype(F32)
        gain = gains[0:1, :] + gains[1:2, :] + gains[2:3, :]
        normed = hat.astype(F32) * gain
        sigma = jax.nn.sigmoid(normed)
        hat_ref[:, cols] = hat
        act_ref[:, cols] = (normed * sigma).astype(BF)
        slope_ref[:, cols] = sigma * (1.0 + normed * (1.0 - sigma)) * gain


def mixed(keep_ref, recv_ref):
    return (keep_ref[...] + recv_ref[...].astype(F32)).astype(BF)


def outer_body(keep_ref, recv_ref, act_ref, own_ref, other_ref, turned_ref):
    mix = mixed(keep_ref, recv_ref)
    turned_ref[...] = jnp.transpose(mix.astype(F32))
    core = lax.rem(lax.axis_index(SP), 2)

    def rows_of(parity):
        return jnp.concatenate(
            [
                turned_ref[pl.ds(pl.multiple_of((2 * b + parity) * 32, 32), 32), :]
                for b in range(8)
            ],
            axis=0,
        ).astype(BF)

    theirs, mine = rows_of(1 - core), rows_of(core)
    for k in range(4):
        act = act_ref[:, k * CH : (k + 1) * CH]
        other_ref[k * 256 : (k + 1) * 256, :] = dot(theirs, act).astype(BF)
        own_ref[k * 256 : (k + 1) * 256, :] = dot(mine, act)


def sum_body(own_ref, recv_ref, out_ref):
    out_ref[...] = (own_ref[...] + recv_ref[...].astype(F32)).astype(BF)


def silu_body(keep_ref, recv_ref, proj_ref, slope_ref, hat_ref, *refs):
    j, _, _ = spot()
    out_refs, part_ref = refs[:4], refs[4]
    mix = mixed(keep_ref, recv_ref)
    part = dot(mix, proj_ref[...])
    sloped = part * slope_ref[...]
    dotted = sloped * hat_ref[...].astype(F32)
    ones = jnp.ones((16, 4 * CH), BF)
    total = dotg(ones, sloped.astype(BF), NT)
    total_dot = dotg(ones, dotted.astype(BF), NT)
    row = lax.broadcasted_iota(jnp.int32, (16, TOK), 0)
    top, top_dot = total.astype(BF).astype(F32), total_dot.astype(BF).astype(F32)
    sums = jnp.where(
        row == 0,
        top,
        jnp.where(
            row == 1,
            total - top,
            jnp.where(row == 2, top_dot, jnp.where(row == 3, total_dot - top_dot, 0.0)),
        ),
    ).astype(BF)
    part_ref[...] = part
    for d, out_ref in enumerate(out_refs):
        out_ref[0:256, :] = part_ref[:, at(lax.rem(j + d, 4) * CH, CH)].astype(BF)
        out_ref[256:272, :] = sums


def conv_body(r0_ref, r1_ref, r2_ref, r3_ref, slope_ref, hat_ref, rstd_ref, out_ref, head_ref):
    j, _, _ = spot()
    recv_refs = (r0_ref, r1_ref, r2_ref, r3_ref)
    total = sum(ref[0:256, :].astype(F32) for ref in recv_refs)
    rows = jnp.concatenate([ref[256:272, :] for ref in recv_refs], axis=0)
    kind = lax.rem(lax.broadcasted_iota(jnp.int32, (64, CH), 0), 16)
    pick = jnp.where(kind < 2, 1.0, 0.0).astype(BF)
    pick_dot = jnp.where(kind < 2, 0.0, jnp.where(kind < 4, 1.0, 0.0)).astype(BF)
    mean = dotg(rows, pick, TN) * (1.0 / (4 * CH))
    mean_dot = dotg(rows, pick_dot, TN) * (1.0 / (4 * CH))
    hat_grad = total * slope_ref[:, at(j * CH, CH)]
    out_ref[...] = rstd_ref[:, 0:1] * (hat_grad - mean - hat_ref[...].astype(F32) * mean_dot)
    head_ref[...] = out_ref[0:32, :]


def taps_body(grad_ref, next_ref, taps_ref, gate_ref, value_ref, out_ref, gate_out_ref, long_ref):
    long_ref[0:256, :] = grad_ref[...]
    long_ref[256:288, :] = next_ref[...]
    for block in range(4):
        row = block * 64
        total = jnp.zeros((64, CH), F32)
        for k in range(31):
            tap = taps_ref[k : k + 1, :].astype(F32)
            total = total + tap * long_ref[row + 30 - k : row + 94 - k, :]
        rows = slice(row, row + 64)
        sigma = jax.nn.sigmoid(gate_ref[rows, :].astype(F32))
        out_ref[rows, :] = (total * sigma).astype(BF)
        gate_out_ref[rows, :] = (
            total * value_ref[rows, :].astype(F32) * sigma * (1.0 - sigma)
        ).astype(BF)


def around(blocks):
    return [lax.ppermute(blocks[d], TP, [(i, (i + d) % 4) for i in range(4)]) for d in (1, 3, 2)]


def exchanged(array, **groups):
    return lax.all_to_all(array, SP, split_axis=0, concat_axis=0, tiled=True, **groups)


def unmix_matrix():
    m = np.zeros((192, 192), np.float32)
    for q in range(4):
        for s in range(8):
            for r in range(6):
                m[q * 48 + s * 6 + r, s * 24 + q * 6 + r] = 1.0
    return m


def on_device(
    moe_input,
    out_cotangent,
    routes,
    group_weight,
    inner_weight,
    gate_weight,
    up_weight,
    down_weight,
    value_in,
    gate_in,
    conv_taps,
    norm_hat,
    norm_rstd,
    norm_gain,
    out_proj,
):
    sp_count = lax.axis_size(SP)
    unmix = unmix_matrix()
    unmix_to = jnp.asarray(unmix, BF)
    unmix_from = jnp.asarray(unmix.T, BF)
    wg, wu, wd = gate_weight[0], up_weight[0], down_weight[0]
    wg2 = lax.ppermute(wg, TP, PAIR_W)
    wu2 = lax.ppermute(wu, TP, PAIR_W)
    wd2 = lax.ppermute(wd, TP, PAIR_W)

    route_weight = group_weight[None, :] * inner_weight.T
    buffer = [pltpu.VMEM((TOK, HALF), BF), pltpu.SemaphoreType.DMA]
    x_send, code_rows = call(
        pack_x_body,
        [((SLOTS, 256), BF), ((2, TOK), jnp.int32)],
        (routes.T, moe_input),
        2 * SLOTS * 1024 * 256,
        vmem=VMEM_WHOLE,
        in_place=(1,),
        scratch=buffer,
    )
    g_send, own_cols = call(
        pack_g_body,
        [((SLOTS, 256), BF), ((TOK, QUART + 128), BF)],
        (code_rows, route_weight, out_cotangent),
        2 * SLOTS * 1024 * 256,
        in_place=(2,),
        scratch=buffer,
    )

    blocks = call(
        aux_body,
        [((AUX, CH), BF)] * 4,
        (out_proj, norm_hat, norm_gain[None, :]),
        0,
    )
    across = lax.ppermute(blocks[1], TP, PAIR_R)
    relayed = lax.ppermute(blocks[3], TP, PAIR_R)
    beside = lax.ppermute(blocks[2], TP, PAIR_W)
    opposite = lax.ppermute(relayed, TP, PAIR_W)
    proj_rows, act, slope, hat, rstd = call(
        channel_body,
        [((512, 4 * CH), BF), ((TOK, 4 * CH), BF), ((TOK, 4 * CH), F32), ((TOK, 4 * CH), BF), ((TOK, 128), F32)],
        (blocks[0], across, beside, opposite, norm_rstd[None, :]),
        0,
    )

    def dispatched(send, parts):
        recv = exchanged(send.reshape(sp_count, 24, 256))
        own = call(
            unpack_body,
            [((ROWS // parts, HALF), BF)] * parts,
            (recv.reshape(SLOTS, 256), unmix_to),
            2 * SLOTS * 192 * 256,
        )
        return own, [lax.ppermute(v, TP, PAIR_R) for v in own]

    (x_own,), (x_other,) = dispatched(x_send, 1)
    g_own, g_other = dispatched(g_send, 2)
    x, *pre = call(
        forward_body,
        [((ROWS, WIDTH), BF)] + [((PART, 2 * HID), F32)] * 4,
        (x_own, x_other, wg, wg2, wu, wu2),
        2 * ROWS * WIDTH * 4 * HID,
        vmem=VMEM_LARGE,
    )
    halves, rows_recv = [], []
    for k in range(2):
        *made, rows_send = call(
            delta_body,
            [((PART, WIDTH), BF)] + [((PART, HID), BF)] * 6 + [((PART, HALF), BF)],
            (g_own[k], g_other[k], pre[2 * k], pre[2 * k + 1], wd, wd2, wg, wg2, wu, wu2),
            2 * PART * WIDTH * 4 * HID,
            in_place=range(4, 10),
            scratch=[pltpu.VMEM((2, HID, WIDTH), BF), pltpu.VMEM((4, HALF, HID), BF)]
            + [pltpu.SemaphoreType.DMA((6,))],
            vmem=VMEM_LARGE,
        )
        halves += made
        rows_recv.append(lax.ppermute(rows_send, TP, PAIR_R))
    g, h, h2, gd, gd2, ud, ud2 = call(
        join_body,
        [((ROWS, WIDTH), BF)] + [((ROWS, HID), BF)] * 6,
        halves,
        0,
    )
    (rows_keep,) = call(
        keep_body,
        [((ROWS, HALF), F32)],
        (gd, gd2, ud, ud2, wg, wg2, wu, wu2),
        2 * ROWS * HALF * 4 * HID,
        vmem=VMEM_LARGE,
    )

    def outer(a, b):
        return lax.dot_general(a, b, TN, preferred_element_type=F32)

    def finished(a, b, b_other):
        other = outer(*b_other).astype(BF)
        arrived = lax.ppermute(other, TP, PAIR_W)
        return (outer(a, b) + arrived.astype(F32)).astype(BF)[None]

    gate_grad = finished(x, gd, (x, gd2))
    up_grad = finished(x, ud, (x, ud2))
    down_own = lax.optimization_barrier(outer(h, g))
    down_arrived = []
    for k in range(2):
        part = outer(h2[:, k * 128 : (k + 1) * 128], g).astype(BF)
        down_arrived.append(lax.ppermute(part, TP, PAIR_W))
    down_grad = (down_own + jnp.concatenate(down_arrived).astype(F32)).astype(BF)[None]

    (back_send,) = call(
        back_pack_body,
        [((SLOTS, 256), BF)],
        (rows_keep, *rows_recv, unmix_from),
        2 * SLOTS * 192 * 256,
    )
    back = exchanged(back_send.reshape(sp_count, 24, 256))

    mix_keep, mix_send = call(
        combine_body,
        [((TOK, QUART), F32), ((TOK, QUART), BF)],
        (back.reshape(SLOTS, 256), own_cols),
        2 * SLOTS * 1024 * 256,
    )
    mix_recv = lax.ppermute(mix_send, TP, PAIR_W)
    outer_own, outer_other = call(
        outer_body,
        [((1024, CH), F32), ((1024, CH), BF)],
        (mix_keep, mix_recv, act),
        2 * TOK * 512 * 1024,
        scratch=[pltpu.VMEM((512, TOK), F32)],
    )
    outer_recv = lax.ppermute(outer_other, SP, [(i, i ^ 1) for i in range(sp_count)])
    (outer_sum,) = call(sum_body, [((1024, CH), BF)], (outer_own, outer_recv), 0)
    pieces = exchanged(
        outer_sum.reshape(sp_count // 2, 32, CH),
        axis_index_groups=[list(range(c, sp_count, 2)) for c in range(2)],
    )
    piece = jnp.sum(pieces.astype(F32), axis=0)
    per_tp = sp_count // 4
    proj_grad = lax.ppermute(
        piece,
        (SP, TP),
        [
            (s * 4 + t, (per_tp * t + s % per_tp) * 4 + s // per_tp)
            for s in range(sp_count)
            for t in range(4)
        ],
    )

    silu_parts = call(
        silu_body,
        [((272, CH), BF)] * 4,
        (mix_keep, mix_recv, proj_rows, slope, hat),
        2 * TOK * 512 * 1024,
        scratch=[pltpu.VMEM((TOK, 4 * CH), F32)],
    )
    silu_parts = [silu_parts[0]] + around(silu_parts)
    conv_grad, head = call(
        conv_body,
        [((TOK, CH), F32), ((32, CH), F32)],
        (*silu_parts, slope, norm_hat, rstd),
        0,
    )
    incoming = lax.ppermute(head, SP, [(i, i - 1) for i in range(1, sp_count)])
    value_grad, gate_in_grad = call(
        taps_body,
        [((TOK, CH), BF), ((TOK, CH), BF)],
        (conv_grad, incoming, conv_taps, gate_in, value_in),
        0,
        scratch=[pltpu.VMEM((TOK + 32, CH), F32)],
    )
    return (gate_grad, up_grad, down_grad, proj_grad, value_grad, gate_in_grad)


def solution(mesh):
    return jax.shard_map(
        on_device,
        mesh=mesh,
        in_specs=(
            P(SP, None),
            P(SP, None),
            P(SP, None),
            P(SP),
            P(SP, None),
            P(SP, None, TP),
            P(SP, None, TP),
            P(SP, TP, None),
            P(SP, TP),
            P(SP, TP),
            P(None, TP),
            P(SP, TP),
            P(SP),
            P(TP),
            P(None, TP),
        ),
        out_specs=(
            P(SP, None, TP),
            P(SP, None, TP),
            P(SP, TP, None),
            P(SP, TP),
            P(SP, TP),
            P(SP, TP),
        ),
        check_vma=False,
    )
```

```python
import jax
import jax.numpy as jnp
import numpy as np
from jax import lax
from jax.experimental import pallas as pl
from jax.experimental.pallas import tpu as pltpu
from jax.sharding import PartitionSpec as P


BF = jnp.bfloat16
F32 = jnp.float32
TOK = 256
WIDTH = 2048
HALF = 1024
QUART = 512
CH = 256
HID = 256
EXPERTS = 64
CAP = 12
SUB = 6
ROWS = 64 * SUB
PART = ROWS // 2
SLOTS = 64 * 24
AUX = 512 + 256 + 16
VMEM_SMALL = 16 * 1024 * 1024
VMEM_LARGE = 24 * 1024 * 1024
VMEM_WHOLE = 60 * 1024 * 1024
SP, TP = "sp", "tp"
PAIR_W = [(0, 1), (1, 0), (2, 3), (3, 2)]
PAIR_R = [(0, 3), (3, 0), (1, 2), (2, 1)]

NT = (((1,), (1,)), ((), ()))
TN = (((0,), (0,)), ((), ()))


def dot(a, b):
    return jnp.dot(a, b, preferred_element_type=F32)


def dotg(a, b, dims):
    return lax.dot_general(a, b, dims, preferred_element_type=F32)


def spot():
    j = lax.axis_index(TP)
    half = lax.shift_right_logical(j, 1)
    row_class = lax.rem(lax.shift_right_logical(j + 1, 1), 2)
    return j, half, row_class


def peers(j):
    return 3 - j, j + 1 - 2 * lax.rem(j, 2), lax.rem(j + 2, 4)


def at(start, size):
    return pl.ds(pl.multiple_of(start, 128), size)


def call(body, outs, args, flops, in_place=(), scratch=(), vmem=VMEM_SMALL):
    bytes_moved = sum(a.size * a.dtype.itemsize for a in args) + sum(
        np.prod(s) * np.dtype(d).itemsize for s, d in outs
    )
    return pl.pallas_call(
        body,
        out_shape=[jax.ShapeDtypeStruct(s, d) for s, d in outs],
        in_specs=[
            pl.BlockSpec(memory_space=pltpu.HBM if i in in_place else pltpu.VMEM)
            for i in range(len(args))
        ],
        out_specs=[pl.BlockSpec(memory_space=pltpu.VMEM)] * len(outs),
        scratch_shapes=list(scratch),
        cost_estimate=pl.CostEstimate(
            flops=int(flops), bytes_accessed=int(bytes_moved), transcendentals=0
        ),
        compiler_params=pltpu.CompilerParams(vmem_limit_bytes=vmem),
    )(*args)


def slot_parts(i):
    who = lax.shift_right_logical(i * 2731, 16)
    rest = i - who * 24
    part = lax.shift_right_logical(rest * 43, 8)
    return who, part, rest - part * 6


def half_copy(from_ref, to_ref, sem, half):
    return pltpu.make_async_copy(from_ref.at[:, at(half * HALF, HALF)], to_ref, sem)


def pick_rows(code_first, code_second, row_class, data, send_ref, weights=None):
    step = 384
    who, part, rank = slot_parts(lax.broadcasted_iota(jnp.int32, (step, TOK), 0))
    base = who * CAP + rank

    def one(k):
        target = base + (k * (step // 24) * CAP + row_class * SUB)
        hit_first = target == code_first
        hit_second = target == code_second
        pick = jnp.where(hit_first, 1.0, jnp.where(hit_second, 1.0, 0.0))
        picks = jnp.concatenate(
            [jnp.where(part == q, pick, 0.0).astype(BF) for q in range(4)], axis=1
        )
        rows = dot(picks, data)
        if weights is not None:
            rows = rows * jnp.sum(
                jnp.where(hit_first, weights[0:1, :], 0.0)
                + jnp.where(hit_second, weights[1:2, :], 0.0),
                axis=1,
                keepdims=True,
            )
        send_ref[pl.ds(pl.multiple_of(k * step, step), step), :] = rows.astype(BF)

    if weights is None:
        for k in range(SLOTS // step):
            one(k)
    else:
        pl.loop(0, SLOTS // step)(one)


def stacked_quarters(buffer):
    return jnp.concatenate([buffer[:, q * 256 : (q + 1) * 256] for q in range(4)], axis=0)


def pack_x_body(routes_ref, input_ref, send_ref, row_ref, buffer, sem):
    _, half, row_class = spot()
    copy = half_copy(input_ref, buffer, sem, half)
    copy.start()
    experts = lax.broadcasted_iota(jnp.int32, (EXPERTS, TOK), 0)
    first, second = routes_ref[0:1, :], routes_ref[1:2, :]
    before = lax.broadcasted_iota(jnp.int32, (TOK, TOK), 0) < lax.broadcasted_iota(
        jnp.int32, (TOK, TOK), 1
    )
    before = jnp.where(before, 1.0, 0.0).astype(BF)
    one_first = jnp.where(experts == first, 1.0, 0.0)
    one_second = jnp.where(experts == second, 1.0, 0.0)
    count_first = dot(one_first.astype(BF), before)
    count_second = dot(one_second.astype(BF), before) + jnp.sum(one_first, axis=1, keepdims=True)
    rank_first = jnp.sum(one_first * count_first, axis=0, keepdims=True).astype(jnp.int32)
    rank_second = jnp.sum(one_second * count_second, axis=0, keepdims=True).astype(jnp.int32)
    code_first = first * CAP + rank_first
    code_second = second * CAP + rank_second
    row_ref[0:1, :] = code_first
    row_ref[1:2, :] = code_second
    copy.wait()
    pick_rows(code_first, code_second, row_class, stacked_quarters(buffer[...]), send_ref)


def pack_g_body(row_ref, weight_ref, grad_ref, send_ref, cols_ref, buffer, sem):
    j, half, row_class = spot()
    copy = half_copy(grad_ref, buffer, sem, half)
    copy.start()
    code_first, code_second = row_ref[0:1, :], row_ref[1:2, :]
    codes = jnp.concatenate(
        [
            jnp.broadcast_to(code_first.astype(F32), (64, TOK)),
            jnp.broadcast_to(code_second.astype(F32), (64, TOK)),
        ],
        axis=0,
    )
    codes = jnp.transpose(codes)
    high = jnp.floor(codes * (1.0 / 256.0))
    lane = lax.broadcasted_iota(jnp.int32, (TOK, 128), 1)
    split = jnp.where(lax.rem(lane, 2) == 0, codes - 256.0 * high, high)
    cols_ref[:, QUART : QUART + 128] = split.astype(BF)
    copy.wait()
    cols_ref[:, 0:QUART] = buffer[:, at(lax.rem(j, 2) * QUART, QUART)]
    pick_rows(
        code_first,
        code_second,
        row_class,
        stacked_quarters(buffer[...]),
        send_ref,
        weight_ref[...],
    )


def unpack_body(recv_ref, perm_ref, *out_refs):
    each = 8 // len(out_refs)
    for group in range(8):
        rows = dot(perm_ref[...], recv_ref[group * 192 : (group + 1) * 192, :]).astype(BF)
        out_ref = out_refs[group // each]
        to = slice(group % each * 48, (group % each + 1) * 48)
        for q in range(4):
            out_ref[to, q * 256 : (q + 1) * 256] = rows[q * 48 : (q + 1) * 48]


def whole_rows(own_ref, other_ref, half, out_ref):
    out_ref[:, at(half * HALF, HALF)] = own_ref[...]
    out_ref[:, at((1 - half) * HALF, HALF)] = other_ref[...]


def forward_body(own_ref, other_ref, wg_ref, wg2_ref, wu_ref, wu2_ref, x_ref, *out_refs):
    _, half, _ = spot()
    whole_rows(own_ref, other_ref, half, x_ref)
    x = x_ref[...]
    for k, w_ref in enumerate((wg_ref, wg2_ref, wu_ref, wu2_ref)):
        made = dot(x, w_ref[...])
        cols = slice(k % 2 * HID, (k % 2 + 1) * HID)
        out_refs[k // 2][:, cols] = made[0:PART]
        out_refs[2 + k // 2][:, cols] = made[PART:ROWS]


def partial_rows(gd, ud, gd2, ud2, wg_ref, wg2_ref, wu_ref, wu2_ref, start):
    rows = at(start, 256)
    return (
        dotg(gd, wg_ref[rows, :], NT)
        + dotg(ud, wu_ref[rows, :], NT)
        + dotg(gd2, wg2_ref[rows, :], NT)
        + dotg(ud2, wu2_ref[rows, :], NT)
    )


def delta_body(
    own_ref, other_ref, gate_ref, up_ref, wd_ref, wd2_ref, wg_ref, wg2_ref, wu_ref, wu2_ref,
    g_ref, h_ref, h2_ref, gd_ref, gd2_ref, ud_ref, ud2_ref, send_ref, down_buf, in_buf, sems,
):
    _, half, _ = spot()
    start = pl.multiple_of((1 - half) * HALF, HALF)
    copies = [
        pltpu.make_async_copy(ref, down_buf.at[k], sems.at[k])
        for k, ref in enumerate((wd_ref, wd2_ref))
    ] + [
        pltpu.make_async_copy(ref.at[pl.ds(start, HALF), :], in_buf.at[k], sems.at[2 + k])
        for k, ref in enumerate((wg_ref, wu_ref, wg2_ref, wu2_ref))
    ]
    for copy in copies:
        copy.start()
    whole_rows(own_ref, other_ref, half, g_ref)
    g = g_ref[...]
    total = jnp.zeros((PART, HALF), F32)
    for k, (ho, go, uo) in enumerate(((h_ref, gd_ref, ud_ref), (h2_ref, gd2_ref, ud2_ref))):
        copies[k].wait()
        act_grad = dotg(g, down_buf[k], NT)
        gate = gate_ref[:, k * HID : (k + 1) * HID]
        up = up_ref[:, k * HID : (k + 1) * HID]
        sigma = jax.nn.sigmoid(gate)
        act = gate * sigma
        ho[...] = (act * up).astype(BF)
        go[...] = (act_grad * up * (sigma * (1.0 + gate * (1.0 - sigma)))).astype(BF)
        uo[...] = (act_grad * act).astype(BF)
    for k, ref in enumerate((gd_ref, ud_ref, gd2_ref, ud2_ref)):
        copies[2 + k].wait()
        total = total + dotg(ref[...], in_buf[k], NT)
    send_ref[...] = total.astype(BF)


def join_body(*refs):
    count = len(refs) // 3
    for k in range(count):
        refs[2 * count + k][0:PART, :] = refs[k][...]
        refs[2 * count + k][PART:ROWS, :] = refs[count + k][...]


def keep_body(gd_ref, gd2_ref, ud_ref, ud2_ref, wg_ref, wg2_ref, wu_ref, wu2_ref, keep_ref):
    _, half, _ = spot()
    deltas = gd_ref[...], ud_ref[...], gd2_ref[...], ud2_ref[...]

    @pl.loop(0, 4)
    def _(k):
        start = half * HALF + k * 256
        keep_ref[:, at(k * 256, 256)] = partial_rows(
            *deltas, wg_ref, wg2_ref, wu_ref, wu2_ref, start
        )


def back_pack_body(keep_ref, first_ref, second_ref, perm_ref, send_ref):
    for group in range(8):
        rows = slice(group * 48, (group + 1) * 48)
        recv_ref = second_ref if group >= 4 else first_ref
        recv = recv_ref[group % 4 * 48 : (group % 4 + 1) * 48, :]
        total = (keep_ref[rows, :] + recv.astype(F32)).astype(BF)
        stacked = jnp.concatenate([total[:, q * 256 : (q + 1) * 256] for q in range(4)], axis=0)
        send_ref[group * 192 : (group + 1) * 192, :] = dot(perm_ref[...], stacked).astype(BF)


def combine_body(back_ref, cols_ref, keep_ref, send_ref):
    j, _, row_class = spot()
    who, part, rank = slot_parts(lax.broadcasted_iota(jnp.int32, (1, SLOTS), 1))
    target = (who * CAP + rank + row_class * SUB).astype(F32)
    codes = cols_ref[:, QUART : QUART + 128].astype(F32)
    code_first = codes[:, 0:1] + 256.0 * codes[:, 1:2]
    code_second = codes[:, 64:65] + 256.0 * codes[:, 65:66]
    hit = jnp.where(target == code_first, 1.0, jnp.where(target == code_second, 1.0, 0.0))
    kept = lax.rem(j, 2) * 2
    back = back_ref[...]
    for a in range(2):
        theirs = dot(jnp.where(part == 2 - kept + a, hit, 0.0).astype(BF), back)
        send_ref[:, a * 256 : (a + 1) * 256] = theirs.astype(BF)
    for a in range(2):
        cols = slice(a * 256, (a + 1) * 256)
        mine = dot(jnp.where(part == kept + a, hit, 0.0).astype(BF), back)
        keep_ref[:, cols] = cols_ref[:, cols].astype(F32) + mine


def aux_body(proj_ref, hat_ref, gain_ref, *out_refs):
    j, _, _ = spot()
    gain = gain_ref[...]
    top = gain.astype(BF)
    rest = gain - top.astype(F32)
    mid = rest.astype(BF)
    low = (rest - mid.astype(F32)).astype(BF)
    row = lax.broadcasted_iota(jnp.int32, (16, CH), 0)
    gains = jnp.where(
        row == 0,
        top.astype(F32),
        jnp.where(row == 1, mid.astype(F32), jnp.where(row == 2, low.astype(F32), 0.0)),
    ).astype(BF)
    for to, out_ref in zip((j, *peers(j)), out_refs):
        out_ref[0:512, :] = proj_ref[pl.ds(pl.multiple_of(to * 512, 512), 512), :]
        out_ref[512:768, :] = hat_ref[...]
        out_ref[768:784, :] = gains


def channel_body(
    own_ref, across_ref, beside_ref, opposite_ref, row_ref, proj_ref, act_ref, slope_ref, hat_ref, rstd_ref
):
    rstd_ref[...] = jnp.transpose(jnp.broadcast_to(row_ref[...], (128, TOK)))
    j, _, _ = spot()
    for owner, ref in zip((j, *peers(j)), (own_ref, across_ref, beside_ref, opposite_ref)):
        cols = at(owner * CH, CH)
        proj_ref[:, cols] = ref[0:512, :]
        hat = ref[512:768, :]
        gains = ref[768:784, :].astype(F32)
        gain = gains[0:1, :] + gains[1:2, :] + gains[2:3, :]
        normed = hat.astype(F32) * gain
        sigma = jax.nn.sigmoid(normed)
        hat_ref[:, cols] = hat
        act_ref[:, cols] = (normed * sigma).astype(BF)
        slope_ref[:, cols] = sigma * (1.0 + normed * (1.0 - sigma)) * gain


def mixed(keep_ref, recv_ref):
    return (keep_ref[...] + recv_ref[...].astype(F32)).astype(BF)


def outer_body(keep_ref, recv_ref, act_ref, own_ref, other_ref, turned_ref):
    mix = mixed(keep_ref, recv_ref)
    turned_ref[...] = jnp.transpose(mix.astype(F32))
    core = lax.rem(lax.axis_index(SP), 2)

    def rows_of(parity):
        return jnp.concatenate(
            [
                turned_ref[pl.ds(pl.multiple_of((2 * b + parity) * 32, 32), 32), :]
                for b in range(8)
            ],
            axis=0,
        ).astype(BF)

    theirs, mine = rows_of(1 - core), rows_of(core)
    for k in range(4):
        act = act_ref[:, k * CH : (k + 1) * CH]
        other_ref[k * 256 : (k + 1) * 256, :] = dot(theirs, act).astype(BF)
        own_ref[k * 256 : (k + 1) * 256, :] = dot(mine, act)


def sum_body(own_ref, recv_ref, out_ref):
    out_ref[...] = (own_ref[...] + recv_ref[...].astype(F32)).astype(BF)


def silu_body(keep_ref, recv_ref, proj_ref, slope_ref, hat_ref, *refs):
    j, _, _ = spot()
    out_refs, part_ref = refs[:4], refs[4]
    mix = mixed(keep_ref, recv_ref)
    part = dot(mix, proj_ref[...])
    sloped = part * slope_ref[...]
    dotted = sloped * hat_ref[...].astype(F32)
    ones = jnp.ones((16, 4 * CH), BF)
    total = dotg(ones, sloped.astype(BF), NT)
    total_dot = dotg(ones, dotted.astype(BF), NT)
    row = lax.broadcasted_iota(jnp.int32, (16, TOK), 0)
    top, top_dot = total.astype(BF).astype(F32), total_dot.astype(BF).astype(F32)
    sums = jnp.where(
        row == 0,
        top,
        jnp.where(
            row == 1,
            total - top,
            jnp.where(row == 2, top_dot, jnp.where(row == 3, total_dot - top_dot, 0.0)),
        ),
    ).astype(BF)
    part_ref[...] = part
    for d, out_ref in enumerate(out_refs):
        out_ref[0:256, :] = part_ref[:, at(lax.rem(j + d, 4) * CH, CH)].astype(BF)
        out_ref[256:272, :] = sums


def conv_body(r0_ref, r1_ref, r2_ref, r3_ref, slope_ref, hat_ref, rstd_ref, out_ref, head_ref):
    j, _, _ = spot()
    recv_refs = (r0_ref, r1_ref, r2_ref, r3_ref)
    total = sum(ref[0:256, :].astype(F32) for ref in recv_refs)
    rows = jnp.concatenate([ref[256:272, :] for ref in recv_refs], axis=0)
    kind = lax.rem(lax.broadcasted_iota(jnp.int32, (64, CH), 0), 16)
    pick = jnp.where(kind < 2, 1.0, 0.0).astype(BF)
    pick_dot = jnp.where(kind < 2, 0.0, jnp.where(kind < 4, 1.0, 0.0)).astype(BF)
    mean = dotg(rows, pick, TN) * (1.0 / (4 * CH))
    mean_dot = dotg(rows, pick_dot, TN) * (1.0 / (4 * CH))
    hat_grad = total * slope_ref[:, at(j * CH, CH)]
    out_ref[...] = rstd_ref[:, 0:1] * (hat_grad - mean - hat_ref[...].astype(F32) * mean_dot)
    head_ref[...] = out_ref[0:32, :]


def taps_body(grad_ref, next_ref, taps_ref, gate_ref, value_ref, out_ref, gate_out_ref, long_ref):
    long_ref[0:256, :] = grad_ref[...]
    long_ref[256:288, :] = next_ref[...]
    for block in range(4):
        row = block * 64
        total = jnp.zeros((64, CH), F32)
        for k in range(31):
            tap = taps_ref[k : k + 1, :].astype(F32)
            total = total + tap * long_ref[row + 30 - k : row + 94 - k, :]
        rows = slice(row, row + 64)
        sigma = jax.nn.sigmoid(gate_ref[rows, :].astype(F32))
        out_ref[rows, :] = (total * sigma).astype(BF)
        gate_out_ref[rows, :] = (
            total * value_ref[rows, :].astype(F32) * sigma * (1.0 - sigma)
        ).astype(BF)


def around(blocks):
    return [lax.ppermute(blocks[d], TP, [(i, (i + d) % 4) for i in range(4)]) for d in (1, 3, 2)]


def exchanged(array, **groups):
    return lax.all_to_all(array, SP, split_axis=0, concat_axis=0, tiled=True, **groups)


def unmix_matrix():
    m = np.zeros((192, 192), np.float32)
    for q in range(4):
        for s in range(8):
            for r in range(6):
                m[q * 48 + s * 6 + r, s * 24 + q * 6 + r] = 1.0
    return m


def on_device(
    moe_input,
    out_cotangent,
    routes,
    group_weight,
    inner_weight,
    gate_weight,
    up_weight,
    down_weight,
    value_in,
    gate_in,
    conv_taps,
    norm_hat,
    norm_rstd,
    norm_gain,
    out_proj,
):
    sp_count = lax.axis_size(SP)
    unmix = unmix_matrix()
    unmix_to = jnp.asarray(unmix, BF)
    unmix_from = jnp.asarray(unmix.T, BF)
    wg, wu, wd = gate_weight[0], up_weight[0], down_weight[0]
    wg2 = lax.ppermute(wg, TP, PAIR_W)
    wu2 = lax.ppermute(wu, TP, PAIR_W)
    wd2 = lax.ppermute(wd, TP, PAIR_W)

    route_weight = group_weight[None, :] * inner_weight.T
    buffer = [pltpu.VMEM((TOK, HALF), BF), pltpu.SemaphoreType.DMA]
    x_send, code_rows = call(
        pack_x_body,
        [((SLOTS, 256), BF), ((2, TOK), jnp.int32)],
        (routes.T, moe_input),
        2 * SLOTS * 1024 * 256,
        vmem=VMEM_WHOLE,
        in_place=(1,),
        scratch=buffer,
    )
    g_send, own_cols = call(
        pack_g_body,
        [((SLOTS, 256), BF), ((TOK, QUART + 128), BF)],
        (code_rows, route_weight, out_cotangent),
        2 * SLOTS * 1024 * 256,
        in_place=(2,),
        scratch=buffer,
    )

    blocks = call(
        aux_body,
        [((AUX, CH), BF)] * 4,
        (out_proj, norm_hat, norm_gain[None, :]),
        0,
    )
    across = lax.ppermute(blocks[1], TP, PAIR_R)
    relayed = lax.ppermute(blocks[3], TP, PAIR_R)
    beside = lax.ppermute(blocks[2], TP, PAIR_W)
    opposite = lax.ppermute(relayed, TP, PAIR_W)
    proj_rows, act, slope, hat, rstd = call(
        channel_body,
        [((512, 4 * CH), BF), ((TOK, 4 * CH), BF), ((TOK, 4 * CH), F32), ((TOK, 4 * CH), BF), ((TOK, 128), F32)],
        (blocks[0], across, beside, opposite, norm_rstd[None, :]),
        0,
    )

    def dispatched(send, parts):
        recv = exchanged(send.reshape(sp_count, 24, 256))
        own = call(
            unpack_body,
            [((ROWS // parts, HALF), BF)] * parts,
            (recv.reshape(SLOTS, 256), unmix_to),
            2 * SLOTS * 192 * 256,
        )
        return own, [lax.ppermute(v, TP, PAIR_R) for v in own]

    (x_own,), (x_other,) = dispatched(x_send, 1)
    g_own, g_other = dispatched(g_send, 2)
    x, *pre = call(
        forward_body,
        [((ROWS, WIDTH), BF)] + [((PART, 2 * HID), F32)] * 4,
        (x_own, x_other, wg, wg2, wu, wu2),
        2 * ROWS * WIDTH * 4 * HID,
        vmem=VMEM_LARGE,
    )
    halves, rows_recv = [], []
    for k in range(2):
        *made, rows_send = call(
            delta_body,
            [((PART, WIDTH), BF)] + [((PART, HID), BF)] * 6 + [((PART, HALF), BF)],
            (g_own[k], g_other[k], pre[2 * k], pre[2 * k + 1], wd, wd2, wg, wg2, wu, wu2),
            2 * PART * WIDTH * 4 * HID,
            in_place=range(4, 10),
            scratch=[pltpu.VMEM((2, HID, WIDTH), BF), pltpu.VMEM((4, HALF, HID), BF)]
            + [pltpu.SemaphoreType.DMA((6,))],
            vmem=VMEM_LARGE,
        )
        halves += made
        rows_recv.append(lax.ppermute(rows_send, TP, PAIR_R))
    g, h, h2, gd, gd2, ud, ud2 = call(
        join_body,
        [((ROWS, WIDTH), BF)] + [((ROWS, HID), BF)] * 6,
        halves,
        0,
    )
    (rows_keep,) = call(
        keep_body,
        [((ROWS, HALF), F32)],
        (gd, gd2, ud, ud2, wg, wg2, wu, wu2),
        2 * ROWS * HALF * 4 * HID,
        vmem=VMEM_LARGE,
    )

    def outer(a, b):
        return lax.dot_general(a, b, TN, preferred_element_type=F32)

    def finished(a, b, b_other):
        other = outer(*b_other).astype(BF)
        arrived = lax.ppermute(other, TP, PAIR_W)
        return (outer(a, b) + arrived.astype(F32)).astype(BF)[None]

    gate_grad = finished(x, gd, (x, gd2))
    up_grad = finished(x, ud, (x, ud2))
    down_own = lax.optimization_barrier(outer(h, g))
    down_arrived = []
    for k in range(2):
        part = outer(h2[:, k * 128 : (k + 1) * 128], g).astype(BF)
        down_arrived.append(lax.ppermute(part, TP, PAIR_W))
    down_grad = (down_own + jnp.concatenate(down_arrived).astype(F32)).astype(BF)[None]

    (back_send,) = call(
        back_pack_body,
        [((SLOTS, 256), BF)],
        (rows_keep, *rows_recv, unmix_from),
        2 * SLOTS * 192 * 256,
    )
    back = exchanged(back_send.reshape(sp_count, 24, 256))

    mix_keep, mix_send = call(
        combine_body,
        [((TOK, QUART), F32), ((TOK, QUART), BF)],
        (back.reshape(SLOTS, 256), own_cols),
        2 * SLOTS * 1024 * 256,
    )
    mix_recv = lax.ppermute(mix_send, TP, PAIR_W)
    outer_own, outer_other = call(
        outer_body,
        [((1024, CH), F32), ((1024, CH), BF)],
        (mix_keep, mix_recv, act),
        2 * TOK * 512 * 1024,
        scratch=[pltpu.VMEM((512, TOK), F32)],
    )
    outer_recv = lax.ppermute(outer_other, SP, [(i, i ^ 1) for i in range(sp_count)])
    (outer_sum,) = call(sum_body, [((1024, CH), BF)], (outer_own, outer_recv), 0)
    pieces = exchanged(
        outer_sum.reshape(sp_count // 2, 32, CH),
        axis_index_groups=[list(range(c, sp_count, 2)) for c in range(2)],
    )
    piece = jnp.sum(pieces.astype(F32), axis=0)
    per_tp = sp_count // 4
    proj_grad = lax.ppermute(
        piece,
        (SP, TP),
        [
            (s * 4 + t, (per_tp * t + s % per_tp) * 4 + s // per_tp)
            for s in range(sp_count)
            for t in range(4)
        ],
    )

    silu_parts = call(
        silu_body,
        [((272, CH), BF)] * 4,
        (mix_keep, mix_recv, proj_rows, slope, hat),
        2 * TOK * 512 * 1024,
        scratch=[pltpu.VMEM((TOK, 4 * CH), F32)],
    )
    silu_parts = [silu_parts[0]] + around(silu_parts)
    conv_grad, head = call(
        conv_body,
        [((TOK, CH), F32), ((32, CH), F32)],
        (*silu_parts, slope, norm_hat, rstd),
        0,
    )
    incoming = lax.ppermute(head, SP, [(i, i - 1) for i in range(1, sp_count)])
    value_grad, gate_in_grad = call(
        taps_body,
        [((TOK, CH), BF), ((TOK, CH), BF)],
        (conv_grad, incoming, conv_taps, gate_in, value_in),
        0,
        scratch=[pltpu.VMEM((TOK + 32, CH), F32)],
    )
    return (gate_grad, up_grad, down_grad, proj_grad, value_grad, gate_in_grad)


def solution(mesh):
    return jax.shard_map(
        on_device,
        mesh=mesh,
        in_specs=(
            P(SP, None),
            P(SP, None),
            P(SP, None),
            P(SP),
            P(SP, None),
            P(SP, None, TP),
            P(SP, None, TP),
            P(SP, TP, None),
            P(SP, TP),
            P(SP, TP),
            P(None, TP),
            P(SP, TP),
            P(SP),
            P(TP),
            P(None, TP),
        ),
        out_specs=(
            P(SP, None, TP),
            P(SP, None, TP),
            P(SP, TP, None),
            P(SP, TP),
            P(SP, TP),
            P(SP, TP),
        ),
        check_vma=False,
    )
```
